32 devices in a mesh: sp: 8 (over z, y), tp: 4 (over x, core).
Axes of the slice: x: 2, y: 2, z: 4, core: 2. Of those that a mesh axis runs over, the one named last changes fastest.
Arguments:
- out_grad: bfloat16 [1024, 2048], P('sp'), may hold values from -6 to 6
- residual: bfloat16 [1024, 2048], P('sp'), may hold values from -6 to 6
- routes: int32 [1024, 2], P('sp'), may hold values from 0 to 3, all different within a row; in each aligned block of 128 rows (0 to 127, 128 to 255, ...) at most 80 rows name the same one
- route_weights: float32 [1024, 2], P('sp'), may hold values from 0.15 to 0.85, as said below
- w_gate: bfloat16 [8, 2048, 2048], P('sp', None, 'tp'), may hold values from -0.125 to 0.125
- w_up: bfloat16 [8, 2048, 2048], P('sp', None, 'tp'), may hold values from -0.125 to 0.125
- w_down: bfloat16 [8, 2048, 2048], P('sp', 'tp'), may hold values from -0.09375 to 0.09375
- out_gate: bfloat16 [1024, 1024], P('sp', 'tp'), may hold values from -6 to 6
- in_gate: bfloat16 [1024, 1024], P('sp', 'tp'), may hold values from -6 to 6
- conv_input: bfloat16 [1024, 1024], P('sp', 'tp'), may hold values from -6 to 6
- conv_out: bfloat16 [1024, 1024], P('sp', 'tp'), may hold values from -6 to 6
- conv_taps: float32 [3, 1024], P(None, 'tp'), may hold values from -3.5 to 3.5
- w_out: bfloat16 [1024, 2048], P('tp'), may hold values from -0.1875 to 0.1875
Outputs:
- grad_resid: bfloat16 [1024, 2048], P('sp')
- grad_up: bfloat16 [8, 2048, 2048], P('sp', None, 'tp')
- grad_down: bfloat16 [8, 2048, 2048], P('sp', 'tp')
- grad_out_gate: bfloat16 [1024, 1024], P('sp', 'tp')
- grad_in_gate: bfloat16 [1024, 1024], P('sp', 'tp')
- grad_conv_input: bfloat16 [1024, 1024], P('sp', 'tp')
- grad_w_out: float32 [2048, 1024], P('sp', 'tp')
The draws below stay inside these ranges and needn't reach their ends.
Inputs may be any that keep to these rules, and one draw needn't show every extreme that they name: `routes`: each row names 2 different experts. In the rows of one index of sp no expert is named more than 80 times, a bound that some block reaches. `route_weights`: the two weights of a row sum to one.
All inputs are finite; a program needn't handle non-finite values.
Results may differ from the reference program's by a relative error of at most 0.013.
Values may be sent and summed in bfloat16 or wider, within the bound.
A program may use at most 128 MiB of HBM per device.

```python
import math
import jax
import jax.numpy as jnp
import numpy as np
from jax import lax

D = 2048
FF_HALF = 2048
SC = 1024
TOP_K = 2
TOK_DEV = 128
TOKENS = 1024
EXPERTS = 4
SLICES = 8
CAP = 80
N_SP = 8
N_TP = 4


def draw_route_weights(key, part):
    leading = jax.random.uniform(key, (TOKENS, 1), jnp.float32, 0.15, 0.85)
    return jnp.concatenate([leading, 1.0 - leading], axis=1)


def with_spikes(array, key, source, target, shards_of, factor):
    owner, partner = [(jnp.arange(array.shape[dim]) // (array.shape[dim] // shards_of)).reshape([-1 if axis == dim else 1 for axis in range(array.ndim)]) for dim in (source, target)]
    chosen = jax.random.permutation(key, shards_of)[partner]
    strong = (owner == chosen) | (owner == (partner + shards_of // 2) % shards_of)
    return jnp.where(strong, factor * array, array)


def steps_of(rng, dims, pieces, least, largest):
    factor_of, own = 1.0, jax.random.fold_in(rng, 6)
    for position, parts in pieces:
        draws = jnp.exp(jax.random.uniform(jax.random.fold_in(own, position), (parts,), jnp.float32, least / len(pieces), largest / len(pieces)))
        factor_of = factor_of * jnp.repeat(draws, dims[position] // parts).reshape([-1 if axis == position else 1 for axis in range(len(dims))])
    return factor_of


def shared_out(own_key, own, number, rows, count, top, reach, lean):
    order = jax.random.permutation(own_key, count)
    heavy_load, usual = load_shares(count, rows * top, reach, lean, True), load_shares(count, rows * top, reach, lean, False)
    places = jnp.arange(count)

    def named(tallies, rotation):
        used = int((tallies > 0).sum())
        fixed = max(1, used // 4)
        passed = fixed + (places - fixed + rotation * (used - fixed)) % max(1, count - fixed)
        return jnp.zeros((count,), jnp.int32).at[order[jnp.where(places < fixed, places, passed)]].set(jnp.asarray(tallies, jnp.int32))

    tallies = jnp.where(number % 4 == 0, named(heavy_load, number // 4), named(usual, number - number // 4 - 1))
    mixed = jax.random.permutation(jax.random.fold_in(own, 3), count)
    source_of, receiver = mixed[0:count // 2 * 2:2], mixed[1:count // 2 * 2:2]
    slack = jnp.minimum(tallies[source_of] - 1, reach - tallies[receiver]) // 2
    slack = jnp.where((source_of == order[0]) | (receiver == order[0]) | (tallies[receiver] == 0), 0, jnp.maximum(slack, 0))
    passed = jax.random.randint(jax.random.fold_in(own, 4), (count // 2,), 0, 1 << 20) % (slack + 1)
    tallies = tallies.at[source_of].add(-passed).at[receiver].add(passed)
    members = jnp.searchsorted(jnp.cumsum(tallies), jnp.arange(rows * top), side="right").astype(jnp.int32)
    grid = members.reshape(top, rows).T
    grid = grid[jax.random.permutation(jax.random.fold_in(own, 1), rows)]
    rotation = jax.random.randint(jax.random.fold_in(own, 2), (rows, 1), 0, top)
    return jnp.take_along_axis(grid, (jnp.arange(top)[None, :] + rotation) % top, axis=1)


def load_shares(amount, total, reach, slope, full):
    portions = [(1 << 20) // math.isqrt(grade ** slope) + 1 for grade in range(1, amount + 1)]
    largest = reach if full else min(reach, max(-(-total // amount), total * portions[0] // sum(portions)))
    least = 1 if total - largest >= amount - 1 else 0
    counts, surplus = [largest] + [least] * (amount - 1), total - largest - least * (amount - 1)
    while surplus > 0:
        candidates = [i for i in range(1, amount) if counts[i] < largest] or [i for i in range(1, amount) if counts[i] < reach]
        whole, remaining = sum([portions[i] for i in candidates]), surplus
        for i in candidates:
            addition = min(reach - counts[i], max(1, remaining * portions[i] // whole), surplus)
            counts[i] = counts[i] + addition
            surplus = surplus - addition
    return np.array(counts)


def scatter_about(key, shape, scale, limit, pieces=(), held_as=jnp.bfloat16):
    entries = scale * jax.random.normal(key, shape, jnp.float32)
    if pieces:
        entries = entries * steps_of(key, shape, pieces, -0.22, 0.18)
    return jnp.clip(entries, -limit, limit).astype(held_as)


def noise_with(stream_key, dims, spread, reach, shards, heavy, kind=jnp.bfloat16):
    entries = spread * jax.random.normal(stream_key, dims, jnp.float32)
    if shards:
        entries = entries * steps_of(stream_key, dims, shards, -0.22, 0.18)
    return jnp.clip(with_spikes(entries, jax.random.fold_in(stream_key, 3), *heavy), -reach, reach).astype(kind)


def setup_inputs(seed: int = 0) -> dict:
    keys = jax.random.split(jax.random.key(seed), 14)
    out_grad = noise_with(keys[0], (TOKENS, D), 1.0, 6.0, ((0, 8),), (0, 1, 8, 2.0))
    residual = scatter_about(keys[1], (TOKENS, D), 1.0, 6.0, ((0, 8),))
    routes_keys = jax.random.split(jax.random.fold_in(keys[2], 1), TOKENS // TOK_DEV)
    routes_turns = jax.random.permutation(jax.random.fold_in(keys[2], 3), TOKENS // TOK_DEV)
    routes = jax.vmap(lambda own, number: shared_out(jax.random.fold_in(keys[2], 2), own, number, TOK_DEV, EXPERTS, TOP_K, CAP, 1))(routes_keys, routes_turns).reshape((TOKENS, TOP_K))
    route_weights = draw_route_weights(jax.random.fold_in(keys[13], 71), 0)
    w_gate = scatter_about(keys[4], (SLICES, D, FF_HALF), D ** -0.5, 0.125, ((0, 8), (2, 4)))
    w_up = scatter_about(keys[5], (SLICES, D, FF_HALF), D ** -0.5, 0.125, ((0, 8), (2, 4)))
    w_down = scatter_about(keys[6], (SLICES, FF_HALF, D), (2 * FF_HALF) ** -0.5, 0.09375, ((0, 8), (1, 4)))
    out_gate = scatter_about(keys[7], (TOKENS, SC), 1.0, 6.0, ((0, 8), (1, 4)))
    in_gate = scatter_about(keys[8], (TOKENS, SC), 1.0, 6.0, ((0, 8), (1, 4)))
    conv_input = scatter_about(keys[9], (TOKENS, SC), 1.0, 6.0, ((0, 8), (1, 4)))
    conv_out = scatter_about(keys[10], (TOKENS, SC), 1.0, 6.0, ((0, 8), (1, 4)))
    conv_taps = scatter_about(keys[11], (3, SC), 3 ** -0.5, 3.5, ((1, 4),), jnp.float32)
    w_out = scatter_about(keys[12], (SC, D), SC ** -0.5, 0.1875, ((0, 4),))
    return dict(out_grad=out_grad, residual=residual, routes=routes, route_weights=route_weights, w_gate=w_gate, w_up=w_up, w_down=w_down, out_gate=out_gate, in_gate=in_gate, conv_input=conv_input, conv_out=conv_out, conv_taps=conv_taps, w_out=w_out)


epsilon = 1e-06

def reference(out_grad, residual, routes, route_weights, w_gate, w_up, w_down, out_gate, in_gate, conv_input, conv_out, conv_taps, w_out):
    resid_f32 = residual.astype(jnp.float32)
    inv_rms = lax.rsqrt(lax.optimization_barrier(jnp.mean(resid_f32 * resid_f32, axis=-1, keepdims=True)) + epsilon)
    unit_rows = resid_f32 * inv_rms
    normed = unit_rows.astype(jnp.bfloat16)
    n_assign = TOKENS * TOP_K
    weighted = (route_weights[:, :, None] * out_grad.astype(jnp.float32)[:, None, :]).astype(jnp.bfloat16).reshape(n_assign, D)
    flat_routes = routes.reshape(-1).astype(jnp.int32)
    onehot = (flat_routes[:, None] == jnp.arange(EXPERTS, dtype=jnp.int32)[None, :]).astype(jnp.int32)
    blocks = onehot.reshape(N_SP, TOP_K * TOK_DEV, EXPERTS)
    before = (jnp.cumsum(blocks, axis=1) - blocks).reshape(n_assign, EXPERTS)
    slot_rank = lax.optimization_barrier(jnp.sum(before * onehot, axis=1)).astype(jnp.int32)
    source = (jnp.arange(n_assign, dtype=jnp.int32) // (TOP_K * TOK_DEV)).astype(jnp.int32)
    slot_table = jnp.full((EXPERTS, N_SP * CAP), n_assign, jnp.int32)
    slot_table = slot_table.at[flat_routes, source * CAP + slot_rank].set(jnp.arange(n_assign, dtype=jnp.int32))
    quarter = FF_HALF // N_TP
    n_blocks = 2 * N_TP

    def one_expert(expert):
        slot_ids = slot_table[expert]
        filled = slot_ids < n_assign
        safe_ids = jnp.where(filled, slot_ids, 0)
        expert_rows = jnp.where(filled[:, None], normed[safe_ids // TOP_K], jnp.zeros((), jnp.bfloat16))
        expert_grads = jnp.where(filled[:, None], weighted[safe_ids], jnp.zeros((), jnp.bfloat16))
        gate_full = jnp.concatenate([w_gate[2 * expert], w_gate[2 * expert + 1]], axis=1)
        up_full = jnp.concatenate([w_up[2 * expert], w_up[2 * expert + 1]], axis=1)
        down_full = jnp.concatenate([w_down[2 * expert], w_down[2 * expert + 1]], axis=0)
        pre_gate = jnp.dot(expert_rows, gate_full, preferred_element_type=jnp.float32)
        pre_up = jnp.dot(expert_rows, up_full, preferred_element_type=jnp.float32)
        sigmoid_gate = jax.nn.sigmoid(pre_gate)
        activated = pre_gate * sigmoid_gate
        hidden = (activated * pre_up).astype(jnp.bfloat16)
        d_hidden = jnp.dot(expert_grads, down_full.T, preferred_element_type=jnp.float32)
        grad_down = jnp.dot(hidden.T, expert_grads, preferred_element_type=jnp.float32).astype(jnp.bfloat16)
        d_gate = (d_hidden * pre_up * sigmoid_gate * (1.0 + pre_gate * (1.0 - sigmoid_gate))).astype(jnp.bfloat16)
        d_up = (d_hidden * activated).astype(jnp.bfloat16)
        grad_up = jnp.dot(expert_rows.T, d_up, preferred_element_type=jnp.float32).astype(jnp.bfloat16)
        partial_value = jnp.einsum('rjf,djf->jrd', d_gate.astype(jnp.float32).reshape(-1, n_blocks, quarter), gate_full.astype(jnp.float32).reshape(D, n_blocks, quarter))
        partial_value = partial_value + jnp.einsum('rjf,djf->jrd', d_up.astype(jnp.float32).reshape(-1, n_blocks, quarter), up_full.astype(jnp.float32).reshape(D, n_blocks, quarter))
        partial_value = lax.optimization_barrier(partial_value.astype(jnp.bfloat16)).astype(jnp.float32)
        slice_sum = lax.optimization_barrier(jnp.sum(partial_value.reshape(2, N_TP, -1, D), axis=1)).astype(jnp.bfloat16)
        down_pair = grad_down.reshape(2, FF_HALF, D)
        up_pair = jnp.transpose(grad_up.reshape(D, 2, FF_HALF), (1, 0, 2))
        return (down_pair, up_pair, slice_sum, slot_ids)
    down_all, up_all, sums_all, ids_all = lax.map(one_expert, jnp.arange(EXPERTS, dtype=jnp.int32))
    grad_down = down_all.reshape(SLICES, FF_HALF, D)
    grad_up = up_all.reshape(SLICES, D, FF_HALF)
    contrib = lax.optimization_barrier(jnp.sum(sums_all.astype(jnp.float32), axis=1)).reshape(-1, D)
    collected = jnp.zeros((n_assign + 1, D), jnp.float32).at[ids_all.reshape(-1)].add(contrib)
    d_normed = lax.optimization_barrier(jnp.sum(collected[:n_assign].reshape(TOKENS, TOP_K, D), axis=1))
    row_mean = lax.optimization_barrier(jnp.mean(unit_rows * d_normed, axis=-1, keepdims=True))
    grad_resid = (out_grad.astype(jnp.float32) + inv_rms * (d_normed - unit_rows * row_mean)).astype(jnp.bfloat16)
    d_mix = jnp.dot(grad_resid, w_out.T, preferred_element_type=jnp.float32)
    conv_f32 = conv_out.astype(jnp.float32)
    gate_f32 = out_gate.astype(jnp.float32)
    grad_out_gate = (d_mix * conv_f32).astype(jnp.bfloat16)
    d_conv = d_mix * gate_f32
    padded = jnp.pad(d_conv, ((1, 1), (0, 0)))
    taps_f32 = conv_taps.astype(jnp.float32)
    d_inner = taps_f32[0] * padded[2:] + taps_f32[1] * padded[1:-1] + taps_f32[2] * padded[:-2]
    grad_in_gate = (d_inner * conv_input.astype(jnp.float32)).astype(jnp.bfloat16)
    grad_conv_input = (d_inner * in_gate.astype(jnp.float32)).astype(jnp.bfloat16)
    mixed = (gate_f32 * conv_f32).astype(jnp.bfloat16)
    grad_w_out = jnp.dot(grad_resid.T, mixed, preferred_element_type=jnp.float32)
    return (grad_resid, grad_up, grad_down, grad_out_gate, grad_in_gate, grad_conv_input, grad_w_out)
```

```python
import functools

import jax
import jax.numpy as jnp
from jax import lax
from jax.experimental import pallas as pl
from jax.experimental.pallas import tpu as pltpu
from jax.sharding import PartitionSpec as P

epsilon = 1e-06


def with_halo(cells, sides, width):
    for axis, dim in sides:
        count = lax.axis_size(axis)
        ends = count - 1
        head = lax.slice_in_dim(cells, 0, width, axis=dim)
        tail = lax.slice_in_dim(cells, cells.shape[dim] - width, cells.shape[dim], axis=dim)
        cells = jnp.concatenate(
            [
                lax.ppermute(tail, axis, [(i, (i + 1) % count) for i in range(ends)]),
                cells,
                lax.ppermute(head, axis, [((i + 1) % count, i) for i in range(ends)]),
            ],
            axis=dim,
        )
    return cells


def per_device_general(
    out_grad,
    residual,
    routes,
    route_weights,
    w_gate,
    w_up,
    w_down,
    out_gate,
    in_gate,
    conv_input,
    conv_out,
    conv_taps,
    w_out,
):
    tok_rows = out_grad.shape[0]
    features = out_grad.shape[1]
    top_count = routes.shape[1]
    slices = lax.axis_size("sp")
    experts = slices // 2
    capacity = 5 * tok_rows // slices
    n_assign = tok_rows * top_count
    resid_f32 = residual.astype(jnp.float32)
    inv_rms = lax.rsqrt(jnp.mean(resid_f32 * resid_f32, axis=-1, keepdims=True) + epsilon)
    unit_rows = resid_f32 * inv_rms
    normed = unit_rows.astype(jnp.bfloat16)
    weighted = (
        (route_weights[:, :, None] * out_grad.astype(jnp.float32)[:, None, :])
        .astype(jnp.bfloat16)
        .reshape(n_assign, features)
    )
    flat_routes = routes.reshape(-1)
    onehot = (flat_routes[:, None] == jnp.arange(experts, dtype=jnp.int32)[None, :]).astype(
        jnp.int32
    )
    slot_rank = jnp.sum((jnp.cumsum(onehot, axis=0) - onehot) * onehot, axis=1)
    slot_index = flat_routes * capacity + slot_rank
    slot_table = (
        jnp.full((experts * capacity,), n_assign, jnp.int32)
        .at[slot_index]
        .set(jnp.arange(n_assign, dtype=jnp.int32))
    )
    filled = slot_table < n_assign
    safe_index = jnp.where(filled, slot_table, 0)
    send_rows = jnp.where(
        filled[:, None], normed[safe_index // top_count], jnp.zeros((), jnp.bfloat16)
    )
    send_grads = jnp.where(filled[:, None], weighted[safe_index], jnp.zeros((), jnp.bfloat16))
    outgoing = jnp.stack([send_rows, send_grads])
    doubled = jnp.repeat(outgoing.reshape(2, experts, capacity, features), 2, axis=1)
    arrived = lax.all_to_all(doubled, "sp", split_axis=1, concat_axis=1, tiled=True)
    expert_rows = arrived[0].reshape(slices * capacity, features)
    expert_grads = arrived[1].reshape(slices * capacity, features)
    gate_local = w_gate[0]
    up_local = w_up[0]
    down_local = w_down[0]
    pre_gate = jnp.dot(expert_rows, gate_local, preferred_element_type=jnp.float32)
    pre_up = jnp.dot(expert_rows, up_local, preferred_element_type=jnp.float32)
    sigmoid_gate = jax.nn.sigmoid(pre_gate)
    activated = pre_gate * sigmoid_gate
    hidden = (activated * pre_up).astype(jnp.bfloat16)
    d_hidden = lax.dot_general(
        expert_grads, down_local, (((1,), (1,)), ((), ())), preferred_element_type=jnp.float32
    )
    grad_down = lax.dot_general(
        hidden, expert_grads, (((0,), (0,)), ((), ())), preferred_element_type=jnp.float32
    ).astype(jnp.bfloat16)
    d_gate = (d_hidden * pre_up * sigmoid_gate * (1.0 + pre_gate * (1.0 - sigmoid_gate))).astype(
        jnp.bfloat16
    )
    d_up = (d_hidden * activated).astype(jnp.bfloat16)
    grad_up = lax.dot_general(
        expert_rows, d_up, (((0,), (0,)), ((), ())), preferred_element_type=jnp.float32
    ).astype(jnp.bfloat16)
    partial_value = lax.dot_general(
        d_gate, gate_local, (((1,), (1,)), ((), ())), preferred_element_type=jnp.float32
    )
    partial_value = partial_value + lax.dot_general(
        d_up, up_local, (((1,), (1,)), ((), ())), preferred_element_type=jnp.float32
    )
    partial_value = partial_value.astype(jnp.bfloat16).reshape(slices, capacity, features)
    summed = lax.psum_scatter(partial_value, "tp", scatter_dimension=2, tiled=True).astype(
        jnp.float32
    )
    returned = lax.all_to_all(
        summed.astype(jnp.bfloat16), "sp", split_axis=0, concat_axis=0, tiled=True
    )
    columns = returned.shape[2]
    flat_back = returned.reshape(slices * capacity, columns)
    first_index = 2 * flat_routes * capacity + slot_rank
    contrib = flat_back[first_index].astype(jnp.float32) + flat_back[first_index + capacity].astype(
        jnp.float32
    )
    d_normed = jnp.sum(contrib.reshape(tok_rows, top_count, columns), axis=1)
    col_start = lax.axis_index("tp") * columns
    unit_part = lax.dynamic_slice_in_dim(unit_rows, col_start, columns, 1)
    grad_part = lax.dynamic_slice_in_dim(out_grad, col_start, columns, 1).astype(jnp.float32)
    row_dots = lax.psum(jnp.sum(unit_part * d_normed, axis=-1), "tp")
    row_mean = row_dots[:, None] / features
    resid_part = (grad_part + inv_rms * (d_normed - unit_part * row_mean)).astype(jnp.bfloat16)
    grad_resid = lax.all_gather(resid_part, "tp", axis=1, tiled=True)
    d_mix = lax.dot_general(
        grad_resid, w_out, (((1,), (1,)), ((), ())), preferred_element_type=jnp.float32
    )
    conv_f32 = conv_out.astype(jnp.float32)
    gate_f32 = out_gate.astype(jnp.float32)
    grad_out_gate = (d_mix * conv_f32).astype(jnp.bfloat16)
    d_conv = d_mix * gate_f32
    padded = with_halo(d_conv.astype(jnp.bfloat16), (("sp", 0),), 1).astype(d_conv.dtype)
    d_inner = conv_taps[0] * padded[2:] + conv_taps[1] * padded[1:-1] + conv_taps[2] * padded[:-2]
    grad_in_gate = (d_inner * conv_input.astype(jnp.float32)).astype(jnp.bfloat16)
    grad_conv_input = (d_inner * in_gate.astype(jnp.float32)).astype(jnp.bfloat16)
    mixed = (gate_f32 * conv_f32).astype(jnp.bfloat16)
    grad_w_out = lax.psum_scatter(
        lax.dot_general(
            grad_resid, mixed, (((0,), (0,)), ((), ())), preferred_element_type=jnp.float32
        ),
        "sp",
        scatter_dimension=0,
        tiled=True,
    )
    return (
        grad_resid,
        grad_up[None],
        grad_down[None],
        grad_out_gate,
        grad_in_gate,
        grad_conv_input,
        grad_w_out,
    )


MESH = pl.DeviceIdType.MESH
BF16 = jnp.bfloat16
F32 = jnp.float32
VMEM_LIMIT = 60 * 1024 * 1024


def place():
    sp, tp = lax.axis_index("sp"), lax.axis_index("tp")
    return sp, tp, lax.div(sp, 2), lax.rem(sp, 2), lax.div(tp, 2), lax.rem(tp, 2)


def greet(peers):
    barrier = pltpu.get_barrier_semaphore()
    for peer in peers:
        pl.semaphore_signal(barrier, inc=1, device_id=peer, device_id_type=MESH)
    return lambda: pl.semaphore_wait(barrier, len(peers))


def columns_of(index, width):
    return pl.ds(pl.multiple_of(index * width, width), width)


def rows_of(index, height):
    return pl.ds(pl.multiple_of(index * height, height), height)


def layer_kernel(
    slices, cap,
    rt_hbm, rw_hbm, resid_hbm, og_hbm, gate_hbm, up_hbm, down_hbm,
    ogate_hbm, igate_hbm, cin_hbm, cout_hbm, taps_hbm, wout_hbm,
    gresid_hbm, gup_hbm, gdown_hbm, gogate_hbm, gigate_hbm, gcin_hbm, gwout_hbm,
    rt, rw, resid, og, gate, up, down, ogate, igate, cin, cout, taps, wout,
    gresid, gup, gdown, gogate, gigate, gcin, gwout,
    rows, grads, hidden, d_gate, d_up, sel, send_rows, send_grads,
    part, sib, pairsum, plane, zsend, ret, dn, edge_out, edge_in, grx, mixed,
    send_sem, recv_sem, in_sem, out_sem,
):
    sp, tp, z, y, x, c = place()
    pairs = slices // 2
    tok, features = resid.shape
    units = gate.shape[1]
    width = features // 4
    sibling = (sp, 2 * x + 1 - c)
    x_peer = (sp, 2 * (1 - x) + c)
    y_peer = (2 * z + 1 - y, tp)
    diagonal = (2 * z + 1 - y, 2 * (1 - x) + c)
    sp_peers = [(lax.rem(sp + k, slices), tp) for k in range(1, slices)]
    ready = greet(sp_peers + [sibling, x_peer, diagonal])

    def pair_of(k):
        pair, bit = 0, 1
        while bit < pairs:
            pair = pair + bit * lax.rem(lax.rem(lax.div(z, bit), 2) + (k // bit) % 2, 2)
            bit *= 2
        return pair

    def fetch(n, src, dst):
        copy = pltpu.make_async_copy(src, dst, in_sem.at[n])
        copy.start()
        return copy

    first = [
        fetch(n, src, dst)
        for n, (src, dst) in enumerate(
            ((resid_hbm, resid), (rt_hbm, rt), (rw_hbm, rw), (og_hbm, og))
        )
    ]
    weights = [
        fetch(4 + n, src, dst)
        for n, (src, dst) in enumerate(((gate_hbm, gate), (up_hbm, up), (down_hbm, down)))
    ]
    gates = [
        fetch(7 + n, src, dst)
        for n, (src, dst) in enumerate(
            (
                (ogate_hbm, ogate), (cout_hbm, cout), (wout_hbm, wout),
                (igate_hbm, igate), (cin_hbm, cin), (taps_hbm, taps),
            )
        )
    ]
    started, stored = [], []

    def send(src, dst, peer):
        n = len(started)
        copy = pltpu.make_async_remote_copy(
            src_ref=src, dst_ref=dst, send_sem=send_sem.at[n], recv_sem=recv_sem.at[n],
            device_id=peer, device_id_type=MESH,
        )
        copy.start()
        started.append(copy)
        return copy

    def store(src, dst):
        copy = pltpu.make_async_copy(src, dst, out_sem.at[len(stored)])
        copy.start()
        stored.append(copy)

    def block(pair, yy, xx, cc):
        return (rows_of(2 * pair + yy, cap), columns_of(2 * xx + cc, width))

    for copy in first:
        copy.wait()
    grid_r = lax.broadcasted_iota(jnp.int32, (tok, tok), 0)
    grid_c = lax.broadcasted_iota(jnp.int32, (tok, tok), 1)
    earlier = (grid_r < grid_c).astype(F32).astype(BF16)
    slot = lax.broadcasted_iota(jnp.int32, (cap, tok), 0).astype(F32)
    r32 = resid[...].astype(F32)
    inv_rms = lax.rsqrt(jnp.mean(r32 * r32, axis=-1, keepdims=True) + epsilon)
    mine = columns_of(tp, width)
    normed = (resid[:, mine].astype(F32) * inv_rms).astype(BF16)
    cot = og[:, mine]

    def choose(e):
        named = (rt[...] == e).astype(F32)
        mask = jnp.sum(named, axis=0, keepdims=True)
        weight = jnp.sum(named * rw[...], axis=0, keepdims=True)
        rank = jnp.dot(
            jnp.broadcast_to(mask, (8, tok)).astype(BF16), earlier, preferred_element_type=F32
        )[0:1]
        pick = jnp.where((rank == slot) & (mask > 0.5), 1.0, 0.0)
        slot_weight = jnp.sum(pick * weight, axis=1, keepdims=True)
        pick = pick.astype(BF16)
        sel[rows_of(e, cap), :] = pick
        return pick, slot_weight

    arriving = {}
    home = block(z, y, x, c)
    for k in range(1, pairs):
        e = pair_of(k)
        pick, slot_weight = choose(e)
        here = rows_of(e, cap)
        send_rows[here, :] = jnp.dot(pick, normed, preferred_element_type=F32).astype(BF16)
        send_grads[here, :] = (
            slot_weight * jnp.dot(pick, cot, preferred_element_type=F32)
        ).astype(BF16)
        if k == 1:
            ready()
        for a, (src, dst) in enumerate(((send_rows, rows), (send_grads, grads))):
            arriving[k, a] = send(src.at[here, :], dst.at[home], (2 * e + y, tp))
    pick, slot_weight = choose(z)
    own_rows = rows_of(sp, cap)
    rows[own_rows, :] = jnp.dot(
        pick, (r32 * inv_rms).astype(BF16), preferred_element_type=F32
    ).astype(BF16)
    grads[own_rows, :] = (
        slot_weight * jnp.dot(pick, og[...], preferred_element_type=F32)
    ).astype(BF16)

    both = (rows, grads)
    outs = [{} for _ in range(pairs)]

    def spread(k):
        out, at = outs[k], block(pair_of(k), y, x, c)
        if k == 0:
            for a, ref in enumerate(both):
                out["y", a] = send(ref.at[at], ref.at[at], y_peer)
            return
        for a, ref in enumerate(both):
            arriving[k, a].wait_recv()
            out["x", a] = send(ref.at[at], ref.at[at], x_peer)
            out["y", a] = send(ref.at[at], ref.at[at], y_peer)
            out["s", a] = send(ref.at[at], ref.at[at], sibling)

    def forward(k):
        out, pair = outs[k], pair_of(k)
        got_x = block(pair, y, 1 - x, c)
        got_y = block(pair, 1 - y, x, c)

        def pass_on(kind, got, a):
            out["s" + kind, a] = send(both[a].at[got], both[a].at[got], sibling)

        if k == 0:
            for a, ref in enumerate(both):
                out["y", a].wait_recv()
                out["d", a] = send(ref.at[got_y], ref.at[got_y], x_peer)
                pass_on("y", got_y, a)
            return
        out["x", 0].wait_recv()
        out["d", 0] = send(rows.at[got_x], rows.at[got_x], y_peer)
        pass_on("x", got_x, 0)
        out["y", 1].wait_recv()
        out["d", 1] = send(grads.at[got_y], grads.at[got_y], x_peer)
        pass_on("y", got_y, 1)
        out["x", 1].wait_recv()
        pass_on("x", got_x, 1)
        out["y", 0].wait_recv()
        pass_on("y", got_y, 0)

    def finish(k):
        out, got = outs[k], block(pair_of(k), 1 - y, 1 - x, c)
        for a, ref in enumerate(both):
            out["d", a].wait_recv()
            out["sd", a] = send(ref.at[got], ref.at[got], sibling)

    def experts(k):
        for kind in ("s", "sx", "sy", "sd"):
            for a in range(2):
                if (kind, a) in outs[k]:
                    outs[k][kind, a].wait_recv()
        at = rows_of(pair_of(k), 2 * cap)
        pre_gate = jnp.dot(rows[at, :], gate[...], preferred_element_type=F32)
        pre_up = jnp.dot(rows[at, :], up[...], preferred_element_type=F32)
        d_hidden = lax.dot_general(
            grads[at, :], down[...], (((1,), (1,)), ((), ())), preferred_element_type=F32
        )
        sigmoid_gate = jax.nn.sigmoid(pre_gate)
        activated = pre_gate * sigmoid_gate
        hidden[at, :] = (activated * pre_up).astype(BF16)
        d_gate[at, :] = (
            d_hidden * pre_up * sigmoid_gate * (1.0 + pre_gate * (1.0 - sigmoid_gate))
        ).astype(BF16)
        d_up[at, :] = (d_hidden * activated).astype(BF16)

    across_units = (((1,), (1,)), ((), ()))
    halves, moved, back = {}, {}, []

    def partials(k):
        at = rows_of(pair_of(k), 2 * cap)
        part[at, :] = (
            lax.dot_general(d_gate[at, :], gate[...], across_units, preferred_element_type=F32)
            + lax.dot_general(d_up[at, :], up[...], across_units, preferred_element_type=F32)
        ).astype(BF16)
        for h in range(2):
            halves[k, h] = send(
                part.at[at, columns_of(2 * h + 1 - c, width)], sib.at[h, at, :], sibling
            )

    def reduce_cores(k):
        pair = pair_of(k)
        at = rows_of(pair, 2 * cap)
        for h in range(2):
            halves[k, h].wait_recv()
            pairsum[h, at, :] = (
                part[at, columns_of(2 * h + c, width)].astype(F32) + sib[h, at, :].astype(F32)
            ).astype(BF16)
        same, other = rows_of(2 * pair + y, cap), rows_of(2 * pair + 1 - y, cap)
        slots = rows_of(pair, cap)
        moved[k] = [
            send(pairsum.at[1 - x, other, :], plane.at[2, slots, :], diagonal),
            send(pairsum.at[1 - x, same, :], plane.at[0, slots, :], x_peer),
            send(pairsum.at[x, other, :], plane.at[1, slots, :], y_peer),
        ]

    def reduce_plane(k):
        pair = pair_of(k)
        slots = rows_of(pair, cap)
        for copy in moved[k]:
            copy.wait_recv()
        total = (
            pairsum[x, rows_of(2 * pair + y, cap), :].astype(F32)
            + plane[0, slots, :].astype(F32)
            + plane[1, slots, :].astype(F32)
            + plane[2, slots, :].astype(F32)
        ).astype(BF16)
        if k:
            zsend[slots, :] = total
            back.append(
                send(zsend.at[slots, :], ret.at[rows_of(z, cap), :], (2 * pair + y, tp))
            )
        else:
            ret[slots, :] = total

    over_rows = (((0,), (0,)), ((), ()))

    def down_chunk(n):
        at = slice(n * units // 2, (n + 1) * units // 2)
        gdown[at, :] = lax.dot_general(
            hidden[:, at], grads[...], over_rows, preferred_element_type=F32
        ).astype(BF16)
        store(gdown.at[at, :], gdown_hbm.at[at, :])

    def up_chunk(n):
        at = slice(n * features // 4, (n + 1) * features // 4)
        gup[at, :] = lax.dot_general(
            rows[:, at], d_up[...], over_rows, preferred_element_type=F32
        ).astype(BF16)
        store(gup.at[at, :], gup_hbm.at[at, :])

    own = rows_of(sp, tok)

    def share_mixed():
        for copy in gates:
            copy.wait()
        mixed[own, :] = (ogate[...].astype(F32) * cout[...].astype(F32)).astype(BF16)
        return [send(mixed.at[own, :], mixed.at[own, :], peer) for peer in sp_peers]

    spread(0)
    forward(0)
    spread(1)
    finish(0)
    forward(1)
    for copy in weights:
        copy.wait()
    experts(0)
    spread(2)
    finish(1)
    partials(0)
    forward(2)
    experts(1)
    for k in range(3, pairs):
        spread(k)
        finish(k - 1)
        partials(k - 2)
        forward(k)
        if k == pairs - 1:
            mixed_copies = share_mixed()
        experts(k - 1)
    finish(pairs - 1)
    reduce_cores(1)
    partials(pairs - 2)
    for k in range(2, pairs - 1):
        reduce_cores(k)
    experts(pairs - 1)
    partials(pairs - 1)
    reduce_plane(1)
    down_chunk(0)
    reduce_cores(pairs - 1)
    reduce_cores(0)
    down_chunk(1)
    for k in range(2, pairs - 1):
        reduce_plane(k)
    up_chunk(0)
    up_chunk(1)
    reduce_plane(pairs - 1)
    reduce_plane(0)
    up_chunk(2)
    up_chunk(3)

    for copy in back:
        copy.wait_recv()
    dn[:, mine] = lax.dot_general(
        sel[...], ret[...], over_rows, preferred_element_type=F32
    ).astype(BF16)
    half = tok // 2
    far = columns_of(2 * (1 - x) + c, width)
    shares, relays = [], []
    for h in range(2):
        at = slice(h * half, (h + 1) * half)
        shares.append(send(dn.at[at, mine], dn.at[at, mine], x_peer))
    near = send(dn.at[:, mine], dn.at[:, mine], sibling)
    for h in range(2):
        at = slice(h * half, (h + 1) * half)
        shares[h].wait_recv()
        relays.append(send(dn.at[at, far], dn.at[at, far], sibling))
    for copy in [near] + relays:
        copy.wait_recv()
    unit = r32 * inv_rms
    d_normed = dn[...].astype(F32)
    row_mean = jnp.mean(unit * d_normed, axis=-1, keepdims=True)
    gresid[...] = (og[...].astype(F32) + inv_rms * (d_normed - unit * row_mean)).astype(BF16)
    share = features // slices
    across = [
        send(
            gresid.at[rows_of(c, half), columns_of(peer[0], share)],
            grx.at[rows_of(2 * sp + c, half), :], peer,
        )
        for peer in sp_peers
    ]
    store(gresid, gresid_hbm)
    d_mix = lax.dot_general(
        gresid[...], wout[...], (((1,), (1,)), ((), ())), preferred_element_type=F32
    )
    d_conv = d_mix * ogate[...].astype(F32)
    edge_out[0] = d_conv[tok - 8 :]
    edge_out[1] = d_conv[:8]
    edges = [
        send(edge_out.at[0], edge_in.at[0], sp_peers[0]),
        send(edge_out.at[1], edge_in.at[1], sp_peers[-1]),
    ]
    gogate[...] = (d_mix * cout[...].astype(F32)).astype(BF16)
    store(gogate, gogate_hbm)
    grx[own, :] = gresid[:, columns_of(sp, share)]
    passed = []
    for n in range(slices - 1):
        across[n].wait_recv()
        got = grx.at[rows_of(2 * lax.rem(sp + slices - 1 - n, slices) + c, half), :]
        passed.append(send(got, got, sibling))
    for copy in edges:
        copy.wait_recv()
    before = jnp.where(sp > 0, edge_in[0, 7:8, :], 0.0)
    after = jnp.where(sp < slices - 1, edge_in[1, 0:1, :], 0.0)
    at = lax.broadcasted_iota(jnp.int32, d_conv.shape, 0)
    later = jnp.where(at == tok - 1, after, pltpu.roll(d_conv, tok - 1, 0))
    former = jnp.where(at == 0, before, pltpu.roll(d_conv, 1, 0))
    d_inner = taps[0:1, :] * later + taps[1:2, :] * d_conv + taps[2:3, :] * former
    gigate[...] = (d_inner * cin[...].astype(F32)).astype(BF16)
    store(gigate, gigate_hbm)
    gcin[...] = (d_inner * igate[...].astype(F32)).astype(BF16)
    store(gcin, gcin_hbm)
    for copy in passed + mixed_copies:
        copy.wait_recv()
    gwout[...] = lax.dot_general(grx[...], mixed[...], over_rows, preferred_element_type=F32)
    store(gwout, gwout_hbm)
    for copy in started:
        copy.wait_send()
    for copy in stored:
        copy.wait()


def layer(slices, cap, args):
    rt, rw, resid, og, gate, up, down, ogate, igate, cin, cout, taps, wout = args
    tok, features = resid.shape
    units, channels = gate.shape[1], ogate.shape[1]
    pairs, width = slices // 2, features // 4
    anywhere = pl.BlockSpec(memory_space=pl.ANY)
    share = features // slices
    outs = (
        (resid.shape, BF16), (gate.shape, BF16), (down.shape, BF16),
        (ogate.shape, BF16), (ogate.shape, BF16), (ogate.shape, BF16), ((share, channels), F32),
    )
    rows = slices * cap
    sems = 26 * pairs + 3 * slices + 8
    return pl.pallas_call(
        functools.partial(layer_kernel, slices, cap),
        out_shape=tuple(jax.ShapeDtypeStruct(*out) for out in outs),
        in_specs=[anywhere] * len(args),
        out_specs=[anywhere] * len(outs),
        scratch_shapes=[pltpu.VMEM(arg.shape, arg.dtype) for arg in args]
        + [pltpu.VMEM(*out) for out in outs]
        + [
            pltpu.VMEM((rows, features), BF16),
            pltpu.VMEM((rows, features), BF16),
            pltpu.VMEM((rows, units), BF16),
            pltpu.VMEM((rows, units), BF16),
            pltpu.VMEM((rows, units), BF16),
            pltpu.VMEM((pairs * cap, tok), BF16),
            pltpu.VMEM((pairs * cap, width), BF16),
            pltpu.VMEM((pairs * cap, width), BF16),
            pltpu.VMEM((rows, features), BF16),
            pltpu.VMEM((2, rows, width), BF16),
            pltpu.VMEM((2, rows, width), BF16),
            pltpu.VMEM((3, pairs * cap, width), BF16),
            pltpu.VMEM((pairs * cap, width), BF16),
            pltpu.VMEM((pairs * cap, width), BF16),
            pltpu.VMEM((tok, features), BF16),
            pltpu.VMEM((2, 8, channels), F32),
            pltpu.VMEM((2, 8, channels), F32),
            pltpu.VMEM((slices * tok, share), BF16),
            pltpu.VMEM((slices * tok, channels), BF16),
            pltpu.SemaphoreType.DMA((sems,)),
            pltpu.SemaphoreType.DMA((sems,)),
            pltpu.SemaphoreType.DMA((len(args),)),
            pltpu.SemaphoreType.DMA((len(outs) + 4,)),
        ],
        compiler_params=pltpu.CompilerParams(
            collective_id=0, has_side_effects=True, vmem_limit_bytes=VMEM_LIMIT
        ),
        name="layer",
    )(*args)


def publish_kernel(count, chunks, *refs):
    srcs, dsts, held = refs[:count], refs[count : 2 * count], refs[2 * count : 3 * count]
    in_sem, out_sem = refs[3 * count :]
    pieces = []
    for src, dst, buf, cut in zip(srcs, dsts, held, chunks):
        height = src.shape[0] // cut
        for n in range(cut):
            at = pl.ds(n * height, height)
            i = len(pieces)
            pieces.append(
                (
                    pltpu.make_async_copy(src.at[at, :], buf.at[at, :], in_sem.at[i]),
                    pltpu.make_async_copy(buf.at[at, :], dst.at[at, :], out_sem.at[i]),
                )
            )
    for take, _ in pieces:
        take.start()
    for take, give in pieces:
        take.wait()
        give.start()
    for _, give in pieces:
        give.wait()


def publish(arrays):
    chunks = [max(1, a.size * a.dtype.itemsize // (512 * 1024)) for a in arrays]
    anywhere = pl.BlockSpec(memory_space=pl.ANY)
    return pl.pallas_call(
        functools.partial(publish_kernel, len(arrays), chunks),
        out_shape=tuple(jax.ShapeDtypeStruct(a.shape, a.dtype) for a in arrays),
        in_specs=[anywhere] * len(arrays),
        out_specs=[anywhere] * len(arrays),
        scratch_shapes=[pltpu.VMEM(a.shape, a.dtype) for a in arrays]
        + [pltpu.SemaphoreType.DMA((sum(chunks),))] * 2,
        compiler_params=pltpu.CompilerParams(vmem_limit_bytes=VMEM_LIMIT),
        name="publish",
    )(*arrays)


def per_device(
    out_grad, residual, routes, route_weights, w_gate, w_up, w_down,
    out_gate, in_gate, conv_input, conv_out, conv_taps, w_out,
):
    slices = lax.axis_size("sp")
    cap = 5 * out_grad.shape[0] // slices
    results = layer(
        slices, cap,
        (
            routes.T, route_weights.T, residual, out_grad, w_gate[0], w_up[0], w_down[0],
            out_gate, in_gate, conv_input, conv_out, conv_taps, w_out,
        ),
    )
    grad_resid, grad_up, grad_down, *small = publish(results)
    return (grad_resid, grad_up[None], grad_down[None], *small)


def fits_kernels(mesh, tokens):
    slices = mesh.shape["sp"]
    rows = tokens // slices
    powers = slices >= 8 and slices & (slices - 1) == 0
    return mesh.shape["tp"] == 4 and powers and (5 * rows // slices) % 16 == 0


def on_device(mesh, out_grad, *rest):
    tokens = out_grad.shape[0] * mesh.shape["sp"]
    body = per_device if fits_kernels(mesh, tokens) else per_device_general
    return body(out_grad, *rest)


def solution(mesh):
    in_specs = (
        P("sp", None),
        P("sp", None),
        P("sp", None),
        P("sp", None),
        P("sp", None, "tp"),
        P("sp", None, "tp"),
        P("sp", "tp", None),
        P("sp", "tp"),
        P("sp", "tp"),
        P("sp", "tp"),
        P("sp", "tp"),
        P(None, "tp"),
        P("tp", None),
    )
    out_specs = (
        P("sp", None),
        P("sp", None, "tp"),
        P("sp", "tp", None),
        P("sp", "tp"),
        P("sp", "tp"),
        P("sp", "tp"),
        P("sp", "tp"),
    )
    return jax.shard_map(
        functools.partial(on_device, mesh), mesh=mesh, in_specs=in_specs, out_specs=out_specs, check_vma=False
    )
```

```python
import functools
import math

import jax
import jax.numpy as jnp
from jax import lax
from jax.experimental import pallas as pl
from jax.experimental.pallas import tpu as pltpu
from jax.sharding import PartitionSpec as P

epsilon = 1e-06


def with_halo(cells, sides, width):
    for axis, dim in sides:
        count = lax.axis_size(axis)
        ends = count - 1
        head = lax.slice_in_dim(cells, 0, width, axis=dim)
        tail = lax.slice_in_dim(cells, cells.shape[dim] - width, cells.shape[dim], axis=dim)
        cells = jnp.concatenate(
            [
                lax.ppermute(tail, axis, [(i, (i + 1) % count) for i in range(ends)]),
                cells,
                lax.ppermute(head, axis, [((i + 1) % count, i) for i in range(ends)]),
            ],
            axis=dim,
        )
    return cells


def per_device_general(
    out_grad,
    residual,
    routes,
    route_weights,
    w_gate,
    w_up,
    w_down,
    out_gate,
    in_gate,
    conv_input,
    conv_out,
    conv_taps,
    w_out,
):
    tok_rows = out_grad.shape[0]
    features = out_grad.shape[1]
    top_count = routes.shape[1]
    slices = lax.axis_size("sp")
    experts = slices // 2
    capacity = 5 * tok_rows // slices
    n_assign = tok_rows * top_count
    resid_f32 = residual.astype(jnp.float32)
    inv_rms = lax.rsqrt(jnp.mean(resid_f32 * resid_f32, axis=-1, keepdims=True) + epsilon)
    unit_rows = resid_f32 * inv_rms
    normed = unit_rows.astype(jnp.bfloat16)
    weighted = (
        (route_weights[:, :, None] * out_grad.astype(jnp.float32)[:, None, :])
        .astype(jnp.bfloat16)
        .reshape(n_assign, features)
    )
    flat_routes = routes.reshape(-1)
    onehot = (flat_routes[:, None] == jnp.arange(experts, dtype=jnp.int32)[None, :]).astype(
        jnp.int32
    )
    slot_rank = jnp.sum((jnp.cumsum(onehot, axis=0) - onehot) * onehot, axis=1)
    slot_index = flat_routes * capacity + slot_rank
    slot_table = (
        jnp.full((experts * capacity,), n_assign, jnp.int32)
        .at[slot_index]
        .set(jnp.arange(n_assign, dtype=jnp.int32))
    )
    filled = slot_table < n_assign
    safe_index = jnp.where(filled, slot_table, 0)
    send_rows = jnp.where(
        filled[:, None], normed[safe_index // top_count], jnp.zeros((), jnp.bfloat16)
    )
    send_grads = jnp.where(filled[:, None], weighted[safe_index], jnp.zeros((), jnp.bfloat16))
    outgoing = jnp.stack([send_rows, send_grads])
    doubled = jnp.repeat(outgoing.reshape(2, experts, capacity, features), 2, axis=1)
    arrived = lax.all_to_all(doubled, "sp", split_axis=1, concat_axis=1, tiled=True)
    expert_rows = arrived[0].reshape(slices * capacity, features)
    expert_grads = arrived[1].reshape(slices * capacity, features)
    gate_local = w_gate[0]
    up_local = w_up[0]
    down_local = w_down[0]
    pre_gate = jnp.dot(expert_rows, gate_local, preferred_element_type=jnp.float32)
    pre_up = jnp.dot(expert_rows, up_local, preferred_element_type=jnp.float32)
    sigmoid_gate = jax.nn.sigmoid(pre_gate)
    activated = pre_gate * sigmoid_gate
    hidden = (activated * pre_up).astype(jnp.bfloat16)
    d_hidden = lax.dot_general(
        expert_grads, down_local, (((1,), (1,)), ((), ())), preferred_element_type=jnp.float32
    )
    grad_down = lax.dot_general(
        hidden, expert_grads, (((0,), (0,)), ((), ())), preferred_element_type=jnp.float32
    ).astype(jnp.bfloat16)
    d_gate = (d_hidden * pre_up * sigmoid_gate * (1.0 + pre_gate * (1.0 - sigmoid_gate))).astype(
        jnp.bfloat16
    )
    d_up = (d_hidden * activated).astype(jnp.bfloat16)
    grad_up = lax.dot_general(
        expert_rows, d_up, (((0,), (0,)), ((), ())), preferred_element_type=jnp.float32
    ).astype(jnp.bfloat16)
    partial_value = lax.dot_general(
        d_gate, gate_local, (((1,), (1,)), ((), ())), preferred_element_type=jnp.float32
    )
    partial_value = partial_value + lax.dot_general(
        d_up, up_local, (((1,), (1,)), ((), ())), preferred_element_type=jnp.float32
    )
    partial_value = partial_value.astype(jnp.bfloat16).reshape(slices, capacity, features)
    summed = lax.psum_scatter(partial_value, "tp", scatter_dimension=2, tiled=True).astype(
        jnp.float32
    )
    returned = lax.all_to_all(
        summed.astype(jnp.bfloat16), "sp", split_axis=0, concat_axis=0, tiled=True
    )
    columns = returned.shape[2]
    flat_back = returned.reshape(slices * capacity, columns)
    first_index = 2 * flat_routes * capacity + slot_rank
    contrib = flat_back[first_index].astype(jnp.float32) + flat_back[first_index + capacity].astype(
        jnp.float32
    )
    d_normed = jnp.sum(contrib.reshape(tok_rows, top_count, columns), axis=1)
    col_start = lax.axis_index("tp") * columns
    unit_part = lax.dynamic_slice_in_dim(unit_rows, col_start, columns, 1)
    grad_part = lax.dynamic_slice_in_dim(out_grad, col_start, columns, 1).astype(jnp.float32)
    row_dots = lax.psum(jnp.sum(unit_part * d_normed, axis=-1), "tp")
    row_mean = row_dots[:, None] / features
    resid_part = (grad_part + inv_rms * (d_normed - unit_part * row_mean)).astype(jnp.bfloat16)
    grad_resid = lax.all_gather(resid_part, "tp", axis=1, tiled=True)
    d_mix = lax.dot_general(
        grad_resid, w_out, (((1,), (1,)), ((), ())), preferred_element_type=jnp.float32
    )
    conv_f32 = conv_out.astype(jnp.float32)
    gate_f32 = out_gate.astype(jnp.float32)
    grad_out_gate = (d_mix * conv_f32).astype(jnp.bfloat16)
    d_conv = d_mix * gate_f32
    padded = with_halo(d_conv.astype(jnp.bfloat16), (("sp", 0),), 1).astype(d_conv.dtype)
    d_inner = conv_taps[0] * padded[2:] + conv_taps[1] * padded[1:-1] + conv_taps[2] * padded[:-2]
    grad_in_gate = (d_inner * conv_input.astype(jnp.float32)).astype(jnp.bfloat16)
    grad_conv_input = (d_inner * in_gate.astype(jnp.float32)).astype(jnp.bfloat16)
    mixed = (gate_f32 * conv_f32).astype(jnp.bfloat16)
    grad_w_out = lax.psum_scatter(
        lax.dot_general(
            grad_resid, mixed, (((0,), (0,)), ((), ())), preferred_element_type=jnp.float32
        ),
        "sp",
        scatter_dimension=0,
        tiled=True,
    )
    return (
        grad_resid,
        grad_up[None],
        grad_down[None],
        grad_out_gate,
        grad_in_gate,
        grad_conv_input,
        grad_w_out,
    )


MESH = pl.DeviceIdType.MESH
BF16 = jnp.bfloat16
F32 = jnp.float32
VMEM_LIMIT = 60 * 1024 * 1024


def place():
    sp, tp = lax.axis_index("sp"), lax.axis_index("tp")
    return sp, tp, lax.div(sp, 2), lax.rem(sp, 2), lax.div(tp, 2), lax.rem(tp, 2)


def greet(peers):
    barrier = pltpu.get_barrier_semaphore()
    for peer in peers:
        pl.semaphore_signal(barrier, inc=1, device_id=peer, device_id_type=MESH)
    return lambda: pl.semaphore_wait(barrier, len(peers))


def columns_of(index, width):
    return pl.ds(pl.multiple_of(index * width, width), width)


def rows_of(index, height):
    return pl.ds(pl.multiple_of(index * height, height), height)


def layer_kernel(
    slices, cap,
    rt_hbm, rw_hbm, resid_hbm, og_hbm, gate_hbm, up_hbm, down_hbm,
    ogate_hbm, igate_hbm, cin_hbm, cout_hbm, taps_hbm, wout_hbm,
    gresid_hbm, gup_hbm, gdown_hbm, gogate_hbm, gigate_hbm, gcin_hbm, gwout_hbm,
    rt, rw, resid, og, gate, up, down, ogate, igate, cin, cout, taps, wout,
    gresid, gup, gdown, gogate, gigate, gcin, gwout,
    rows, grads, hidden, d_gate, d_up, sel, send_rows, send_grads,
    part, sib, pairsum, plane, zsend, ret, dn, edge_out, edge_in, grx, mixed,
    send_sem, recv_sem, in_sem, out_sem,
):
    sp, tp, z, y, x, c = place()
    pairs = slices // 2
    tok, features = resid.shape
    units = gate.shape[1]
    width = features // 4
    sibling = (sp, 2 * x + 1 - c)
    x_peer = (sp, 2 * (1 - x) + c)
    y_peer = (2 * z + 1 - y, tp)
    diagonal = (2 * z + 1 - y, 2 * (1 - x) + c)
    sp_peers = [(lax.rem(sp + k, slices), tp) for k in range(1, slices)]
    ready = greet(sp_peers + [sibling, x_peer, diagonal])

    def pair_of(k):
        pair, bit = 0, 1
        while bit < pairs:
            pair = pair + bit * lax.rem(lax.rem(lax.div(z, bit), 2) + (k // bit) % 2, 2)
            bit *= 2
        return pair

    def fetch(n, src, dst):
        copy = pltpu.make_async_copy(src, dst, in_sem.at[n])
        copy.start()
        return copy

    first = [
        fetch(n, src, dst)
        for n, (src, dst) in enumerate(
            ((resid_hbm, resid), (rt_hbm, rt), (rw_hbm, rw), (og_hbm, og))
        )
    ]
    weights = [
        fetch(4 + n, src, dst)
        for n, (src, dst) in enumerate(((gate_hbm, gate), (up_hbm, up), (down_hbm, down)))
    ]
    gates = [
        fetch(7 + n, src, dst)
        for n, (src, dst) in enumerate(
            (
                (ogate_hbm, ogate), (cout_hbm, cout), (wout_hbm, wout),
                (igate_hbm, igate), (cin_hbm, cin), (taps_hbm, taps),
            )
        )
    ]
    stored, unit_cols = [], gate.shape[1]
    slots_used, leaving = [0], [[]]

    def units_of(ref):
        return math.prod(ref.shape) * jnp.dtype(ref.dtype).itemsize // (2 * unit_cols)

    def await_units(sem, units):
        assert units <= gate.shape[0]
        like = gate.at[pl.ds(0, units), :]
        pltpu.make_async_copy(like, like, sem).wait()

    class Batch:
        def __init__(self):
            self.slot, self.units = slots_used[0], 0
            slots_used[0] += 1

        def wait_recv(self):
            await_units(recv_sem.at[self.slot], self.units)

    def send(src, dst, peer, batch=None):
        batch = batch or Batch()
        units = units_of(src)
        batch.units += units
        if sum(leaving[-1]) + units > gate.shape[0]:
            leaving.append([])
        leaving[-1].append(units)
        pltpu.make_async_remote_copy(
            src_ref=src, dst_ref=dst, send_sem=send_sem.at[len(leaving) - 1],
            recv_sem=recv_sem.at[batch.slot], device_id=peer, device_id_type=MESH,
        ).start()
        return batch

    def store(src, dst):
        copy = pltpu.make_async_copy(src, dst, out_sem.at[len(stored)])
        copy.start()
        stored.append(copy)

    def block(pair, yy, xx, cc):
        return (rows_of(2 * pair + yy, cap), columns_of(2 * xx + cc, width))

    for copy in first:
        copy.wait()
    grid_r = lax.broadcasted_iota(jnp.int32, (tok, tok), 0)
    grid_c = lax.broadcasted_iota(jnp.int32, (tok, tok), 1)
    earlier = (grid_r < grid_c).astype(F32).astype(BF16)
    slot = lax.broadcasted_iota(jnp.int32, (cap, tok), 0).astype(F32)
    r32 = resid[...].astype(F32)
    inv_rms = lax.rsqrt(jnp.mean(r32 * r32, axis=-1, keepdims=True) + epsilon)
    mine = columns_of(tp, width)
    normed = (resid[:, mine].astype(F32) * inv_rms).astype(BF16)
    cot = og[:, mine]

    def choose(e):
        named = (rt[...] == e).astype(F32)
        mask = jnp.sum(named, axis=0, keepdims=True)
        weight = jnp.sum(named * rw[...], axis=0, keepdims=True)
        rank = jnp.dot(
            jnp.broadcast_to(mask, (8, tok)).astype(BF16), earlier, preferred_element_type=F32
        )[0:1]
        pick = jnp.where((rank == slot) & (mask > 0.5), 1.0, 0.0)
        slot_weight = jnp.sum(pick * weight, axis=1, keepdims=True)
        pick = pick.astype(BF16)
        sel[rows_of(e, cap), :] = pick
        return pick, slot_weight

    arriving = {}
    home = block(z, y, x, c)
    for k in range(1, pairs):
        e = pair_of(k)
        pick, slot_weight = choose(e)
        here = rows_of(e, cap)
        send_rows[here, :] = jnp.dot(pick, normed, preferred_element_type=F32).astype(BF16)
        send_grads[here, :] = (
            slot_weight * jnp.dot(pick, cot, preferred_element_type=F32)
        ).astype(BF16)
        if k == 1:
            ready()
        for a, (src, dst) in enumerate(((send_rows, rows), (send_grads, grads))):
            arriving[k, a] = send(src.at[here, :], dst.at[home], (2 * e + y, tp))
    pick, slot_weight = choose(z)
    own_rows = rows_of(sp, cap)
    rows[own_rows, :] = jnp.dot(
        pick, (r32 * inv_rms).astype(BF16), preferred_element_type=F32
    ).astype(BF16)
    grads[own_rows, :] = (
        slot_weight * jnp.dot(pick, og[...], preferred_element_type=F32)
    ).astype(BF16)

    both = (rows, grads)
    outs = [{} for _ in range(pairs)]
    near_rows = [Batch() for _ in range(pairs)]

    def spread(k, a):
        out, ref, at = outs[k], both[a], block(pair_of(k), y, x, c)
        if k:
            arriving[k, a].wait_recv()
            out["x", a] = send(ref.at[at], ref.at[at], x_peer)
        out["y", a] = send(ref.at[at], ref.at[at], y_peer)
        if k:
            send(ref.at[at], ref.at[at], sibling, near_rows[k])

    def got_x(k, a):
        out, ref, at = outs[k], both[a], block(pair_of(k), y, 1 - x, c)
        out["x", a].wait_recv()
        if a == 0:
            out["d", a] = send(ref.at[at], ref.at[at], y_peer)
        send(ref.at[at], ref.at[at], sibling, near_rows[k])

    def got_y(k, a):
        out, ref, at = outs[k], both[a], block(pair_of(k), 1 - y, x, c)
        out["y", a].wait_recv()
        if k == 0 or a == 1:
            out["d", a] = send(ref.at[at], ref.at[at], x_peer)
        send(ref.at[at], ref.at[at], sibling, near_rows[k])

    def got_d(k, a):
        out, ref, at = outs[k], both[a], block(pair_of(k), 1 - y, 1 - x, c)
        out["d", a].wait_recv()
        send(ref.at[at], ref.at[at], sibling, near_rows[k])

    across_units = (((1,), (1,)), ((), ()))
    held, halves, moved, back = {}, {}, {}, Batch()

    def experts(k, step):
        at = rows_of(pair_of(k), 2 * cap)
        if step == 0:
            near_rows[k].wait_recv()
            held["gate"] = jnp.dot(rows[at, :], gate[...], preferred_element_type=F32)
        elif step == 1:
            held["up"] = jnp.dot(rows[at, :], up[...], preferred_element_type=F32)
        else:
            pre_gate, pre_up = held["gate"], held["up"]
            d_hidden = lax.dot_general(
                grads[at, :], down[...], across_units, preferred_element_type=F32
            )
            sigmoid_gate = jax.nn.sigmoid(pre_gate)
            activated = pre_gate * sigmoid_gate
            hidden[at, :] = (activated * pre_up).astype(BF16)
            d_gate[at, :] = (
                d_hidden * pre_up * sigmoid_gate * (1.0 + pre_gate * (1.0 - sigmoid_gate))
            ).astype(BF16)
            d_up[at, :] = (d_hidden * activated).astype(BF16)

    def partials(k, h):
        at = rows_of(pair_of(k), 2 * cap)
        cols = slice(2 * h * width, 2 * (h + 1) * width)
        part[at, cols] = (
            lax.dot_general(
                d_gate[at, :], gate[cols, :], across_units, preferred_element_type=F32
            )
            + lax.dot_general(d_up[at, :], up[cols, :], across_units, preferred_element_type=F32)
        ).astype(BF16)
        halves[k, h] = send(
            part.at[at, columns_of(2 * h + 1 - c, width)], sib.at[h, at, :], sibling
        )

    def reduce_cores(k):
        pair = pair_of(k)
        at = rows_of(pair, 2 * cap)
        for h in range(2):
            halves[k, h].wait_recv()
            pairsum[h, at, :] = (
                part[at, columns_of(2 * h + c, width)].astype(F32) + sib[h, at, :].astype(F32)
            ).astype(BF16)
        same, other = rows_of(2 * pair + y, cap), rows_of(2 * pair + 1 - y, cap)
        slots = rows_of(pair, cap)
        moved[k] = Batch()
        for n, src, peer in (
            (2, pairsum.at[1 - x, other, :], diagonal),
            (0, pairsum.at[1 - x, same, :], x_peer),
            (1, pairsum.at[x, other, :], y_peer),
        ):
            send(src, plane.at[n, slots, :], peer, moved[k])

    def reduce_plane(k):
        pair = pair_of(k)
        slots = rows_of(pair, cap)
        moved[k].wait_recv()
        total = (
            pairsum[x, rows_of(2 * pair + y, cap), :].astype(F32)
            + plane[0, slots, :].astype(F32)
            + plane[1, slots, :].astype(F32)
            + plane[2, slots, :].astype(F32)
        ).astype(BF16)
        if k:
            zsend[slots, :] = total
            send(zsend.at[slots, :], ret.at[rows_of(z, cap), :], (2 * pair + y, tp), back)
        else:
            ret[slots, :] = total

    over_rows = (((0,), (0,)), ((), ()))

    def down_chunk(n):
        at = slice(n * units // 2, (n + 1) * units // 2)
        gdown[at, :] = lax.dot_general(
            hidden[:, at], grads[...], over_rows, preferred_element_type=F32
        ).astype(BF16)
        store(gdown.at[at, :], gdown_hbm.at[at, :])

    def up_chunk(n):
        at = slice(n * features // 4, (n + 1) * features // 4)
        gup[at, :] = lax.dot_general(
            rows[:, at], d_up[...], over_rows, preferred_element_type=F32
        ).astype(BF16)
        store(gup.at[at, :], gup_hbm.at[at, :])

    own = rows_of(sp, tok)

    mixed_z, mixed_y = Batch(), Batch()

    def share_mixed():
        for copy in gates:
            copy.wait()
        mixed[own, :] = (ogate[...].astype(F32) * cout[...].astype(F32)).astype(BF16)
        for k in range(1, pairs):
            peer = (2 * pair_of(k) + y, tp)
            send(mixed.at[own, :], mixed.at[own, :], peer, mixed_z)

    def relay_mixed():
        mixed_z.wait_recv()
        for k in range(pairs):
            at = rows_of(2 * pair_of(k) + y, tok)
            send(mixed.at[at, :], mixed.at[at, :], y_peer, mixed_y)

    for a in range(2):
        spread(0, a)
    for a in range(2):
        got_y(0, a)
        spread(1, a)
    for copy in weights:
        copy.wait()
    for k in range(1, pairs):
        if k == 1:
            got_d(0, 0)
        got_y(k, 0)
        if k == 1:
            got_x(k, 0)
            got_y(k, 1)
            got_d(0, 1)
        if k + 1 < pairs:
            spread(k + 1, 0)
        experts(k - 1, 0)
        if k > 1:
            got_y(k, 1)
            got_x(k, 0)
        elif k + 1 < pairs:
            spread(k + 1, 1)
        experts(k - 1, 1)
        if 1 < k < pairs - 1:
            spread(k + 1, 1)
        got_x(k, 1)
        if k + 2 == pairs:
            share_mixed()
        experts(k - 1, 2)
        partials(k - 1, 0)
        got_d(k, 0)
        got_d(k, 1)
        partials(k - 1, 1)
    for k in range(1, pairs - 1):
        reduce_cores(k)
    for step in range(3):
        experts(pairs - 1, step)
    for h in range(2):
        partials(pairs - 1, h)
    reduce_plane(1)
    down_chunk(0)
    reduce_cores(pairs - 1)
    reduce_cores(0)
    down_chunk(1)
    for k in range(2, pairs - 1):
        reduce_plane(k)
    up_chunk(0)
    up_chunk(1)
    reduce_plane(pairs - 1)
    reduce_plane(0)
    relay_mixed()

    back.wait_recv()
    dn[:, mine] = lax.dot_general(
        sel[...], ret[...], over_rows, preferred_element_type=F32
    ).astype(BF16)
    half, quarter = tok // 2, tok // 4
    far = columns_of(2 * (1 - x) + c, width)
    tops = [slice(h * half, (h + 1) * half) for h in range(2)]
    shares = [send(dn.at[at, mine], dn.at[at, mine], x_peer) for at in tops]
    near = [send(dn.at[at, mine], dn.at[at, mine], sibling) for at in tops]
    share = features // slices
    across = []

    def share_rows(h):
        shares[h].wait_recv()
        send(dn.at[tops[h], far], dn.at[tops[h], far], sibling, near[h])
        if h == 0:
            up_chunk(2)
        near[h].wait_recv()

    def resid_rows(h):
        at = tops[h]
        unit = r32[at] * inv_rms[at]
        d_normed = dn[at, :].astype(F32)
        row_mean = jnp.mean(unit * d_normed, axis=-1, keepdims=True)
        gresid[at, :] = (
            og[at, :].astype(F32) + inv_rms[at] * (d_normed - unit * row_mean)
        ).astype(BF16)
        for peer in sp_peers:
            across.append(
                send(
                    gresid.at[rows_of(2 * h + c, quarter), columns_of(peer[0], share)],
                    grx.at[rows_of(4 * sp + 2 * h + c, quarter), :], peer,
                )
            )

    share_rows(0)
    resid_rows(0)
    share_rows(1)
    resid_rows(1)
    store(gresid, gresid_hbm)
    d_mix = lax.dot_general(
        gresid[...], wout[...], (((1,), (1,)), ((), ())), preferred_element_type=F32
    )
    d_conv = d_mix * ogate[...].astype(F32)
    edge_out[0] = d_conv[tok - 8 :]
    edge_out[1] = d_conv[:8]
    edges, passed = Batch(), Batch()
    send(edge_out.at[0], edge_in.at[0], sp_peers[0], edges)
    send(edge_out.at[1], edge_in.at[1], sp_peers[-1], edges)
    gogate[...] = (d_mix * cout[...].astype(F32)).astype(BF16)
    store(gogate, gogate_hbm)
    grx[own, :] = gresid[:, columns_of(sp, share)]
    up_chunk(3)
    for h in range(2):
        for n in range(slices - 1):
            across[h * (slices - 1) + n].wait_recv()
            origin = lax.rem(sp + slices - 1 - n, slices)
            got = grx.at[rows_of(4 * origin + 2 * h + c, quarter), :]
            send(got, got, sibling, passed)
    edges.wait_recv()
    before = jnp.where(sp > 0, edge_in[0, 7:8, :], 0.0)
    after = jnp.where(sp < slices - 1, edge_in[1, 0:1, :], 0.0)
    at = lax.broadcasted_iota(jnp.int32, d_conv.shape, 0)
    later = jnp.where(at == tok - 1, after, pltpu.roll(d_conv, tok - 1, 0))
    former = jnp.where(at == 0, before, pltpu.roll(d_conv, 1, 0))
    d_inner = taps[0:1, :] * later + taps[1:2, :] * d_conv + taps[2:3, :] * former
    gigate[...] = (d_inner * cin[...].astype(F32)).astype(BF16)
    store(gigate, gigate_hbm)
    gcin[...] = (d_inner * igate[...].astype(F32)).astype(BF16)
    store(gcin, gcin_hbm)
    passed.wait_recv()
    mixed_y.wait_recv()
    gwout[...] = lax.dot_general(grx[...], mixed[...], over_rows, preferred_element_type=F32)
    store(gwout, gwout_hbm)
    for n, units in enumerate(leaving):
        await_units(send_sem.at[n], sum(units))
    for copy in stored:
        copy.wait()
    assert slots_used[0] == recv_sem.shape[0] and len(leaving) <= send_sem.shape[0]


def layer(slices, cap, args):
    rt, rw, resid, og, gate, up, down, ogate, igate, cin, cout, taps, wout = args
    tok, features = resid.shape
    units, channels = gate.shape[1], ogate.shape[1]
    pairs, width = slices // 2, features // 4
    anywhere = pl.BlockSpec(memory_space=pl.ANY)
    share = features // slices
    outs = (
        (resid.shape, BF16), (gate.shape, BF16), (down.shape, BF16),
        (ogate.shape, BF16), (ogate.shape, BF16), (ogate.shape, BF16), ((share, channels), F32),
    )
    rows = slices * cap
    sems = 12 * pairs + 2 * slices + 3
    return pl.pallas_call(
        functools.partial(layer_kernel, slices, cap),
        out_shape=tuple(jax.ShapeDtypeStruct(*out) for out in outs),
        in_specs=[anywhere] * len(args),
        out_specs=[anywhere] * len(outs),
        scratch_shapes=[pltpu.VMEM(arg.shape, arg.dtype) for arg in args]
        + [pltpu.VMEM(*out) for out in outs]
        + [
            pltpu.VMEM((rows, features), BF16),
            pltpu.VMEM((rows, features), BF16),
            pltpu.VMEM((rows, units), BF16),
            pltpu.VMEM((rows, units), BF16),
            pltpu.VMEM((rows, units), BF16),
            pltpu.VMEM((pairs * cap, tok), BF16),
            pltpu.VMEM((pairs * cap, width), BF16),
            pltpu.VMEM((pairs * cap, width), BF16),
            pltpu.VMEM((rows, features), BF16),
            pltpu.VMEM((2, rows, width), BF16),
            pltpu.VMEM((2, rows, width), BF16),
            pltpu.VMEM((3, pairs * cap, width), BF16),
            pltpu.VMEM((pairs * cap, width), BF16),
            pltpu.VMEM((pairs * cap, width), BF16),
            pltpu.VMEM((tok, features), BF16),
            pltpu.VMEM((2, 8, channels), F32),
            pltpu.VMEM((2, 8, channels), F32),
            pltpu.VMEM((slices * tok, share), BF16),
            pltpu.VMEM((slices * tok, channels), BF16),
            pltpu.SemaphoreType.DMA((5,)),
            pltpu.SemaphoreType.DMA((sems,)),
            pltpu.SemaphoreType.DMA((len(args),)),
            pltpu.SemaphoreType.DMA((len(outs) + 4,)),
        ],
        compiler_params=pltpu.CompilerParams(
            collective_id=0, has_side_effects=True, vmem_limit_bytes=VMEM_LIMIT
        ),
        name="layer",
    )(*args)


def publish_kernel(count, chunks, *refs):
    srcs, dsts, held = refs[:count], refs[count : 2 * count], refs[2 * count : 3 * count]
    in_sem, out_sem = refs[3 * count :]
    pieces = []
    for src, dst, buf, cut in zip(srcs, dsts, held, chunks):
        height = src.shape[0] // cut
        for n in range(cut):
            at = pl.ds(n * height, height)
            i = len(pieces)
            pieces.append(
                (
                    pltpu.make_async_copy(src.at[at, :], buf.at[at, :], in_sem.at[i]),
                    pltpu.make_async_copy(buf.at[at, :], dst.at[at, :], out_sem.at[i]),
                )
            )
    for take, _ in pieces:
        take.start()
    for take, give in pieces:
        take.wait()
        give.start()
    for _, give in pieces:
        give.wait()


def publish(arrays):
    chunks = [max(1, a.size * a.dtype.itemsize // (512 * 1024)) for a in arrays]
    anywhere = pl.BlockSpec(memory_space=pl.ANY)
    return pl.pallas_call(
        functools.partial(publish_kernel, len(arrays), chunks),
        out_shape=tuple(jax.ShapeDtypeStruct(a.shape, a.dtype) for a in arrays),
        in_specs=[anywhere] * len(arrays),
        out_specs=[anywhere] * len(arrays),
        scratch_shapes=[pltpu.VMEM(a.shape, a.dtype) for a in arrays]
        + [pltpu.SemaphoreType.DMA((sum(chunks),))] * 2,
        compiler_params=pltpu.CompilerParams(vmem_limit_bytes=VMEM_LIMIT),
        name="publish",
    )(*arrays)


def per_device(
    out_grad, residual, routes, route_weights, w_gate, w_up, w_down,
    out_gate, in_gate, conv_input, conv_out, conv_taps, w_out,
):
    slices = lax.axis_size("sp")
    cap = 5 * out_grad.shape[0] // slices
    results = layer(
        slices, cap,
        (
            routes.T, route_weights.T, residual, out_grad, w_gate[0], w_up[0], w_down[0],
            out_gate, in_gate, conv_input, conv_out, conv_taps, w_out,
        ),
    )
    grad_resid, grad_up, grad_down, *small = publish(results)
    return (grad_resid, grad_up[None], grad_down[None], *small)


def fits_kernels(mesh, tokens):
    slices = mesh.shape["sp"]
    rows = tokens // slices
    powers = slices >= 8 and slices & (slices - 1) == 0
    return mesh.shape["tp"] == 4 and powers and (5 * rows // slices) % 16 == 0


def on_device(mesh, out_grad, *rest):
    tokens = out_grad.shape[0] * mesh.shape["sp"]
    body = per_device if fits_kernels(mesh, tokens) else per_device_general
    return body(out_grad, *rest)


def solution(mesh):
    in_specs = (
        P("sp", None),
        P("sp", None),
        P("sp", None),
        P("sp", None),
        P("sp", None, "tp"),
        P("sp", None, "tp"),
        P("sp", "tp", None),
        P("sp", "tp"),
        P("sp", "tp"),
        P("sp", "tp"),
        P("sp", "tp"),
        P(None, "tp"),
        P("tp", None),
    )
    out_specs = (
        P("sp", None),
        P("sp", None, "tp"),
        P("sp", "tp", None),
        P("sp", "tp"),
        P("sp", "tp"),
        P("sp", "tp"),
        P("sp", "tp"),
    )
    return jax.shard_map(
        functools.partial(on_device, mesh), mesh=mesh, in_specs=in_specs, out_specs=out_specs, check_vma=False
    )
```

```python
import functools
import math

import jax
import jax.numpy as jnp
from jax import lax
from jax.experimental import pallas as pl
from jax.experimental.pallas import tpu as pltpu
from jax.sharding import PartitionSpec as P

epsilon = 1e-06


def with_halo(cells, sides, width):
    for axis, dim in sides:
        count = lax.axis_size(axis)
        ends = count - 1
        head = lax.slice_in_dim(cells, 0, width, axis=dim)
        tail = lax.slice_in_dim(cells, cells.shape[dim] - width, cells.shape[dim], axis=dim)
        cells = jnp.concatenate(
            [
                lax.ppermute(tail, axis, [(i, (i + 1) % count) for i in range(ends)]),
                cells,
                lax.ppermute(head, axis, [((i + 1) % count, i) for i in range(ends)]),
            ],
            axis=dim,
        )
    return cells


def per_device_general(
    out_grad,
    residual,
    routes,
    route_weights,
    w_gate,
    w_up,
    w_down,
    out_gate,
    in_gate,
    conv_input,
    conv_out,
    conv_taps,
    w_out,
):
    tok_rows = out_grad.shape[0]
    features = out_grad.shape[1]
    top_count = routes.shape[1]
    slices = lax.axis_size("sp")
    experts = slices // 2
    capacity = 5 * tok_rows // slices
    n_assign = tok_rows * top_count
    resid_f32 = residual.astype(jnp.float32)
    inv_rms = lax.rsqrt(jnp.mean(resid_f32 * resid_f32, axis=-1, keepdims=True) + epsilon)
    unit_rows = resid_f32 * inv_rms
    normed = unit_rows.astype(jnp.bfloat16)
    weighted = (
        (route_weights[:, :, None] * out_grad.astype(jnp.float32)[:, None, :])
        .astype(jnp.bfloat16)
        .reshape(n_assign, features)
    )
    flat_routes = routes.reshape(-1)
    onehot = (flat_routes[:, None] == jnp.arange(experts, dtype=jnp.int32)[None, :]).astype(
        jnp.int32
    )
    slot_rank = jnp.sum((jnp.cumsum(onehot, axis=0) - onehot) * onehot, axis=1)
    slot_index = flat_routes * capacity + slot_rank
    slot_table = (
        jnp.full((experts * capacity,), n_assign, jnp.int32)
        .at[slot_index]
        .set(jnp.arange(n_assign, dtype=jnp.int32))
    )
    filled = slot_table < n_assign
    safe_index = jnp.where(filled, slot_table, 0)
    send_rows = jnp.where(
        filled[:, None], normed[safe_index // top_count], jnp.zeros((), jnp.bfloat16)
    )
    send_grads = jnp.where(filled[:, None], weighted[safe_index], jnp.zeros((), jnp.bfloat16))
    outgoing = jnp.stack([send_rows, send_grads])
    doubled = jnp.repeat(outgoing.reshape(2, experts, capacity, features), 2, axis=1)
    arrived = lax.all_to_all(doubled, "sp", split_axis=1, concat_axis=1, tiled=True)
    expert_rows = arrived[0].reshape(slices * capacity, features)
    expert_grads = arrived[1].reshape(slices * capacity, features)
    gate_local = w_gate[0]
    up_local = w_up[0]
    down_local = w_down[0]
    pre_gate = jnp.dot(expert_rows, gate_local, preferred_element_type=jnp.float32)
    pre_up = jnp.dot(expert_rows, up_local, preferred_element_type=jnp.float32)
    sigmoid_gate = jax.nn.sigmoid(pre_gate)
    activated = pre_gate * sigmoid_gate
    hidden = (activated * pre_up).astype(jnp.bfloat16)
    d_hidden = lax.dot_general(
        expert_grads, down_local, (((1,), (1,)), ((), ())), preferred_element_type=jnp.float32
    )
    grad_down = lax.dot_general(
        hidden, expert_grads, (((0,), (0,)), ((), ())), preferred_element_type=jnp.float32
    ).astype(jnp.bfloat16)
    d_gate = (d_hidden * pre_up * sigmoid_gate * (1.0 + pre_gate * (1.0 - sigmoid_gate))).astype(
        jnp.bfloat16
    )
    d_up = (d_hidden * activated).astype(jnp.bfloat16)
    grad_up = lax.dot_general(
        expert_rows, d_up, (((0,), (0,)), ((), ())), preferred_element_type=jnp.float32
    ).astype(jnp.bfloat16)
    partial_value = lax.dot_general(
        d_gate, gate_local, (((1,), (1,)), ((), ())), preferred_element_type=jnp.float32
    )
    partial_value = partial_value + lax.dot_general(
        d_up, up_local, (((1,), (1,)), ((), ())), preferred_element_type=jnp.float32
    )
    partial_value = partial_value.astype(jnp.bfloat16).reshape(slices, capacity, features)
    summed = lax.psum_scatter(partial_value, "tp", scatter_dimension=2, tiled=True).astype(
        jnp.float32
    )
    returned = lax.all_to_all(
        summed.astype(jnp.bfloat16), "sp", split_axis=0, concat_axis=0, tiled=True
    )
    columns = returned.shape[2]
    flat_back = returned.reshape(slices * capacity, columns)
    first_index = 2 * flat_routes * capacity + slot_rank
    contrib = flat_back[first_index].astype(jnp.float32) + flat_back[first_index + capacity].astype(
        jnp.float32
    )
    d_normed = jnp.sum(contrib.reshape(tok_rows, top_count, columns), axis=1)
    col_start = lax.axis_index("tp") * columns
    unit_part = lax.dynamic_slice_in_dim(unit_rows, col_start, columns, 1)
    grad_part = lax.dynamic_slice_in_dim(out_grad, col_start, columns, 1).astype(jnp.float32)
    row_dots = lax.psum(jnp.sum(unit_part * d_normed, axis=-1), "tp")
    row_mean = row_dots[:, None] / features
    resid_part = (grad_part + inv_rms * (d_normed - unit_part * row_mean)).astype(jnp.bfloat16)
    grad_resid = lax.all_gather(resid_part, "tp", axis=1, tiled=True)
    d_mix = lax.dot_general(
        grad_resid, w_out, (((1,), (1,)), ((), ())), preferred_element_type=jnp.float32
    )
    conv_f32 = conv_out.astype(jnp.float32)
    gate_f32 = out_gate.astype(jnp.float32)
    grad_out_gate = (d_mix * conv_f32).astype(jnp.bfloat16)
    d_conv = d_mix * gate_f32
    padded = with_halo(d_conv.astype(jnp.bfloat16), (("sp", 0),), 1).astype(d_conv.dtype)
    d_inner = conv_taps[0] * padded[2:] + conv_taps[1] * padded[1:-1] + conv_taps[2] * padded[:-2]
    grad_in_gate = (d_inner * conv_input.astype(jnp.float32)).astype(jnp.bfloat16)
    grad_conv_input = (d_inner * in_gate.astype(jnp.float32)).astype(jnp.bfloat16)
    mixed = (gate_f32 * conv_f32).astype(jnp.bfloat16)
    grad_w_out = lax.psum_scatter(
        lax.dot_general(
            grad_resid, mixed, (((0,), (0,)), ((), ())), preferred_element_type=jnp.float32
        ),
        "sp",
        scatter_dimension=0,
        tiled=True,
    )
    return (
        grad_resid,
        grad_up[None],
        grad_down[None],
        grad_out_gate,
        grad_in_gate,
        grad_conv_input,
        grad_w_out,
    )


MESH = pl.DeviceIdType.MESH
BF16 = jnp.bfloat16
F32 = jnp.float32
VMEM_LIMIT = 60 * 1024 * 1024


def place():
    sp, tp = lax.axis_index("sp"), lax.axis_index("tp")
    return sp, tp, lax.div(sp, 2), lax.rem(sp, 2), lax.div(tp, 2), lax.rem(tp, 2)


def greet(peers):
    barrier = pltpu.get_barrier_semaphore()
    for peer in peers:
        pl.semaphore_signal(barrier, inc=1, device_id=peer, device_id_type=MESH)
    return lambda: pl.semaphore_wait(barrier, len(peers))


def columns_of(index, width):
    return pl.ds(pl.multiple_of(index * width, width), width)


def rows_of(index, height):
    return pl.ds(pl.multiple_of(index * height, height), height)


def layer_kernel(
    slices, cap,
    rt_hbm, rw_hbm, resid_hbm, og_hbm, gate_hbm, up_hbm, down_hbm,
    ogate_hbm, igate_hbm, cin_hbm, cout_hbm, taps_hbm, wout_hbm,
    gresid, gup, gdown, gogate, gigate, gcin, gwout,
    rt, rw, resid, og, gate, up, down, ogate, igate, cin, cout, taps, wout,
    rows, grads, hidden, d_gate, d_up, sel, send_rows, send_grads,
    part, sib, pairsum, plane, zsend, ret, dn, edge_out, edge_in, grx, mixed,
    send_sem, recv_sem, in_sem,
):
    sp, tp, z, y, x, c = place()
    pairs = slices // 2
    tok, features = resid.shape
    units = gate.shape[1]
    width = features // 4
    sibling = (sp, 2 * x + 1 - c)
    x_peer = (sp, 2 * (1 - x) + c)
    y_peer = (2 * z + 1 - y, tp)
    diagonal = (2 * z + 1 - y, 2 * (1 - x) + c)
    sp_peers = [(lax.rem(sp + k, slices), tp) for k in range(1, slices)]
    ready = greet(sp_peers + [sibling, x_peer, diagonal])

    def pair_of(k):
        code, pair, bit = k ^ (k >> 1), 0, 1
        while bit < pairs:
            pair = pair + bit * lax.rem(lax.rem(lax.div(z, bit), 2) + (code // bit) % 2, 2)
            bit *= 2
        return pair

    def fetch(n, src, dst):
        copy = pltpu.make_async_copy(src, dst, in_sem.at[n])
        copy.start()
        return copy

    first = [
        fetch(n, src, dst)
        for n, (src, dst) in enumerate(
            ((resid_hbm, resid), (rt_hbm, rt), (rw_hbm, rw), (og_hbm, og))
        )
    ]
    weights = [
        fetch(4 + n, src, dst)
        for n, (src, dst) in enumerate(((gate_hbm, gate), (up_hbm, up), (down_hbm, down)))
    ]
    gates = [
        fetch(7 + n, src, dst)
        for n, (src, dst) in enumerate(
            (
                (ogate_hbm, ogate), (cout_hbm, cout), (wout_hbm, wout),
                (igate_hbm, igate), (cin_hbm, cin), (taps_hbm, taps),
            )
        )
    ]
    unit_cols = gate.shape[1]
    slots_used, leaving = [0], [[]]

    def units_of(ref):
        return math.prod(ref.shape) * jnp.dtype(ref.dtype).itemsize // (2 * unit_cols)

    def await_units(sem, units):
        assert units <= gate.shape[0]
        like = gate.at[pl.ds(0, units), :]
        pltpu.make_async_copy(like, like, sem).wait()

    class Batch:
        def __init__(self):
            self.slot, self.units = slots_used[0], 0
            slots_used[0] += 1

        def wait_recv(self):
            await_units(recv_sem.at[self.slot], self.units)

    def send(src, dst, peer, batch=None):
        batch = batch or Batch()
        units = units_of(src)
        batch.units += units
        if sum(leaving[-1]) + units > gate.shape[0]:
            leaving.append([])
        leaving[-1].append(units)
        pltpu.make_async_remote_copy(
            src_ref=src, dst_ref=dst, send_sem=send_sem.at[len(leaving) - 1],
            recv_sem=recv_sem.at[batch.slot], device_id=peer, device_id_type=MESH,
        ).start()
        return batch

    def block(pair, yy, xx, cc):
        return (rows_of(2 * pair + yy, cap), columns_of(2 * xx + cc, width))

    for copy in first:
        copy.wait()
    grid_r = lax.broadcasted_iota(jnp.int32, (tok, tok), 0)
    grid_c = lax.broadcasted_iota(jnp.int32, (tok, tok), 1)
    earlier = (grid_r < grid_c).astype(F32).astype(BF16)
    slot = lax.broadcasted_iota(jnp.int32, (cap, tok), 0).astype(F32)
    r32 = resid[...].astype(F32)
    inv_rms = lax.rsqrt(jnp.mean(r32 * r32, axis=-1, keepdims=True) + epsilon)
    mine = columns_of(tp, width)
    normed = (resid[:, mine].astype(F32) * inv_rms).astype(BF16)
    cot = og[:, mine]

    def choose(e):
        named = (rt[...] == e).astype(F32)
        mask = jnp.sum(named, axis=0, keepdims=True)
        weight = jnp.sum(named * rw[...], axis=0, keepdims=True)
        rank = jnp.dot(
            jnp.broadcast_to(mask, (8, tok)).astype(BF16), earlier, preferred_element_type=F32
        )[0:1]
        pick = jnp.where((rank == slot) & (mask > 0.5), 1.0, 0.0)
        slot_weight = jnp.sum(pick * weight, axis=1, keepdims=True)
        pick = pick.astype(BF16)
        sel[rows_of(e, cap), :] = pick
        return pick, slot_weight

    both, arriving = (rows, grads), {}
    outs = [{} for _ in range(pairs)]
    near_rows = [Batch() for _ in range(pairs)]

    def spread(k, a):
        out, ref, at = outs[k], both[a], block(pair_of(k), y, x, c)
        if k:
            arriving[k, a].wait_recv()
            out["x", a] = send(ref.at[at], ref.at[at], x_peer)
        out["y", a] = send(ref.at[at], ref.at[at], y_peer)
        if k:
            send(ref.at[at], ref.at[at], sibling, near_rows[k])

    def dispatch(k):
        e = pair_of(k)
        pick, slot_weight = choose(e)
        here, home = rows_of(e, cap), block(z, y, x, c)
        send_rows[here, :] = jnp.dot(pick, normed, preferred_element_type=F32).astype(BF16)
        arriving[k, 0] = send(send_rows.at[here, :], rows.at[home], (2 * e + y, tp))
        send_grads[here, :] = (
            slot_weight * jnp.dot(pick, cot, preferred_element_type=F32)
        ).astype(BF16)
        arriving[k, 1] = send(send_grads.at[here, :], grads.at[home], (2 * e + y, tp))

    pick, slot_weight = choose(z)
    own_rows = rows_of(sp, cap)
    rows[own_rows, :] = jnp.dot(
        pick, (r32 * inv_rms).astype(BF16), preferred_element_type=F32
    ).astype(BF16)
    ready()
    spread(0, 0)
    dispatch(1)
    grads[own_rows, :] = (
        slot_weight * jnp.dot(pick, og[...], preferred_element_type=F32)
    ).astype(BF16)
    spread(0, 1)
    for k in range(2, pairs):
        dispatch(k)

    def got_x(k, a):
        out, ref, at = outs[k], both[a], block(pair_of(k), y, 1 - x, c)
        out["x", a].wait_recv()
        if a == 0:
            out["d", a] = send(ref.at[at], ref.at[at], y_peer)
        send(ref.at[at], ref.at[at], sibling, near_rows[k])

    def got_y(k, a):
        out, ref, at = outs[k], both[a], block(pair_of(k), 1 - y, x, c)
        out["y", a].wait_recv()
        if k == 0 or a == 1:
            out["d", a] = send(ref.at[at], ref.at[at], x_peer)
        send(ref.at[at], ref.at[at], sibling, near_rows[k])

    def got_d(k, a):
        out, ref, at = outs[k], both[a], block(pair_of(k), 1 - y, 1 - x, c)
        out["d", a].wait_recv()
        send(ref.at[at], ref.at[at], sibling, near_rows[k])

    across_units = (((1,), (1,)), ((), ()))
    held, halves, moved, back = {}, {}, {}, Batch()

    def experts(k, step):
        at = rows_of(pair_of(k), 2 * cap)
        if step == 0:
            near_rows[k].wait_recv()
            held["gate"] = jnp.dot(rows[at, :], gate[...], preferred_element_type=F32)
        elif step == 1:
            held["up"] = jnp.dot(rows[at, :], up[...], preferred_element_type=F32)
        else:
            pre_gate, pre_up = held["gate"], held["up"]
            d_hidden = lax.dot_general(
                grads[at, :], down[...], across_units, preferred_element_type=F32
            )
            sigmoid_gate = jax.nn.sigmoid(pre_gate)
            activated = pre_gate * sigmoid_gate
            hidden[at, :] = (activated * pre_up).astype(BF16)
            d_gate[at, :] = (
                d_hidden * pre_up * sigmoid_gate * (1.0 + pre_gate * (1.0 - sigmoid_gate))
            ).astype(BF16)
            d_up[at, :] = (d_hidden * activated).astype(BF16)

    def partials(k, step):
        at, h = rows_of(pair_of(k), 2 * cap), x if step else 1 - x
        cols = columns_of(h, 2 * width)
        part[at, cols] = (
            lax.dot_general(
                d_gate[at, :], gate[cols, :], across_units, preferred_element_type=F32
            )
            + lax.dot_general(d_up[at, :], up[cols, :], across_units, preferred_element_type=F32)
        ).astype(BF16)
        halves[k, step] = send(
            part.at[at, columns_of(2 * h + 1 - c, width)], sib.at[h, at, :], sibling
        )

    def reduce_cores(k, step):
        pair, h = pair_of(k), x if step else 1 - x
        at = rows_of(pair, 2 * cap)
        halves[k, step].wait_recv()
        pairsum[h, at, :] = (
            part[at, columns_of(2 * h + c, width)].astype(F32) + sib[h, at, :].astype(F32)
        ).astype(BF16)
        same, other = rows_of(2 * pair + y, cap), rows_of(2 * pair + 1 - y, cap)
        slots = rows_of(pair, cap)
        if step:
            send(pairsum.at[h, other, :], plane.at[1, slots, :], y_peer, moved[k])
        else:
            moved[k] = Batch()
            send(pairsum.at[h, other, :], plane.at[2, slots, :], diagonal, moved[k])
            send(pairsum.at[h, same, :], plane.at[0, slots, :], x_peer, moved[k])

    def reduce_plane(k):
        pair = pair_of(k)
        slots = rows_of(pair, cap)
        moved[k].wait_recv()
        total = (
            pairsum[x, rows_of(2 * pair + y, cap), :].astype(F32)
            + plane[0, slots, :].astype(F32)
            + plane[1, slots, :].astype(F32)
            + plane[2, slots, :].astype(F32)
        ).astype(BF16)
        if k:
            zsend[slots, :] = total
            send(zsend.at[slots, :], ret.at[rows_of(z, cap), :], (2 * pair + y, tp), back)
        else:
            ret[slots, :] = total

    over_rows = (((0,), (0,)), ((), ()))

    def down_chunk(n):
        at = slice(n * units // 2, (n + 1) * units // 2)
        gdown[at, :] = lax.dot_general(
            hidden[:, at], grads[...], over_rows, preferred_element_type=F32
        ).astype(BF16)

    def up_chunk(n):
        at = slice(n * features // 4, (n + 1) * features // 4)
        gup[at, :] = lax.dot_general(
            rows[:, at], d_up[...], over_rows, preferred_element_type=F32
        ).astype(BF16)

    own = rows_of(sp, tok)

    mixed_z, mixed_y = Batch(), Batch()

    def share_mixed():
        for copy in gates:
            copy.wait()
        mixed[own, :] = (ogate[...].astype(F32) * cout[...].astype(F32)).astype(BF16)
        for k in range(1, pairs):
            peer = (2 * pair_of(k) + y, tp)
            send(mixed.at[own, :], mixed.at[own, :], peer, mixed_z)

    def relay_mixed():
        mixed_z.wait_recv()
        for k in range(pairs):
            at = rows_of(2 * pair_of(k) + y, tok)
            send(mixed.at[at, :], mixed.at[at, :], y_peer, mixed_y)

    for a in range(2):
        got_y(0, a)
        spread(1, a)
    for copy in weights:
        copy.wait()
    for k in range(1, pairs):
        if k == 1:
            got_d(0, 0)
        got_y(k, 0)
        if k == 1:
            got_x(k, 0)
            got_y(k, 1)
            got_d(0, 1)
        if k + 1 < pairs:
            spread(k + 1, 0)
        experts(k - 1, 0)
        if k > 1:
            got_y(k, 1)
            got_x(k, 0)
        elif k + 1 < pairs:
            spread(k + 1, 1)
        experts(k - 1, 1)
        if 1 < k < pairs - 1:
            spread(k + 1, 1)
        got_x(k, 1)
        if k + 2 == pairs:
            share_mixed()
        if k + 1 == pairs:
            for n in range(1, k - 1):
                reduce_cores(n, 0)
                reduce_cores(n, 1)
        experts(k - 1, 2)
        partials(k - 1, 0)
        got_d(k, 0)
        got_d(k, 1)
        partials(k - 1, 1)
    last = pairs - 1
    experts(last, 0)
    reduce_cores(last - 1, 0)
    experts(last, 1)
    reduce_cores(last - 1, 1)
    experts(last, 2)
    partials(last, 0)
    partials(last, 1)
    for k in range(1, last - 1):
        reduce_plane(k)
    up_chunk(0)
    reduce_cores(last, 0)
    reduce_cores(last, 1)
    reduce_cores(0, 0)
    reduce_cores(0, 1)
    reduce_plane(last - 1)
    up_chunk(1)
    down_chunk(0)
    down_chunk(1)
    up_chunk(2)
    up_chunk(3)
    reduce_plane(last)
    reduce_plane(0)
    relay_mixed()

    back.wait_recv()
    dn[:, mine] = lax.dot_general(
        sel[...], ret[...], over_rows, preferred_element_type=F32
    ).astype(BF16)
    half, quarter = tok // 2, tok // 4
    far = columns_of(2 * (1 - x) + c, width)
    share = features // slices
    shares, near, across, crossed = [], [], [], []
    for h in (1 - x, x):
        at = rows_of(h, half)
        shares.append(send(dn.at[at, mine], dn.at[at, mine], x_peer))
    for h in (x, 1 - x):
        at = rows_of(h, half)
        near.append(send(dn.at[at, mine], dn.at[at, mine], sibling))

    def share_rows(step):
        at = rows_of(1 - x if step else x, half)
        shares[step].wait_recv()
        send(dn.at[at, far], dn.at[at, far], sibling, near[step])
        near[step].wait_recv()

    def resid_rows(step):
        at = rows_of(1 - x if step else x, half)
        r_part = resid[at, :].astype(F32)
        inv_part = lax.rsqrt(jnp.mean(r_part * r_part, axis=-1, keepdims=True) + epsilon)
        unit = r_part * inv_part
        d_normed = dn[at, :].astype(F32)
        row_mean = jnp.mean(unit * d_normed, axis=-1, keepdims=True)
        gresid[at, :] = (
            og[at, :].astype(F32) + inv_part * (d_normed - unit * row_mean)
        ).astype(BF16)

    def piece(origin, xx):
        return grx.at[rows_of(4 * origin + 2 * xx + c, quarter), :]

    share_rows(0)
    resid_rows(0)
    for peer in sp_peers:
        src = gresid.at[rows_of(2 * x + c, quarter), columns_of(peer[0], share)]
        across.append(send(src, piece(sp, x), peer))
    share_rows(1)
    resid_rows(1)
    d_mix = lax.dot_general(
        gresid[...], wout[...], (((1,), (1,)), ((), ())), preferred_element_type=F32
    )
    d_conv = d_mix * ogate[...].astype(F32)
    edge_out[0] = d_conv[tok - 8 :]
    edge_out[1] = d_conv[:8]
    edges, passed = Batch(), Batch()
    send(edge_out.at[0], edge_in.at[0], sp_peers[0], edges)
    send(edge_out.at[1], edge_in.at[1], sp_peers[-1], edges)
    gogate[...] = (d_mix * cout[...].astype(F32)).astype(BF16)
    grx[own, :] = gresid[:, columns_of(sp, share)]
    origins = [lax.rem(sp + slices - 1 - n, slices) for n in range(slices - 1)]
    for n, origin in enumerate(origins):
        across[n].wait_recv()
        got = piece(origin, x)
        crossed.append(send(got, got, x_peer))
        send(got, got, sibling, passed)
    for n, origin in enumerate(origins):
        crossed[n].wait_recv()
        got = piece(origin, 1 - x)
        send(got, got, sibling, passed)
    edges.wait_recv()
    before = jnp.where(sp > 0, edge_in[0, 7:8, :], 0.0)
    after = jnp.where(sp < slices - 1, edge_in[1, 0:1, :], 0.0)
    at = lax.broadcasted_iota(jnp.int32, d_conv.shape, 0)
    later = jnp.where(at == tok - 1, after, pltpu.roll(d_conv, tok - 1, 0))
    former = jnp.where(at == 0, before, pltpu.roll(d_conv, 1, 0))
    d_inner = taps[0:1, :] * later + taps[1:2, :] * d_conv + taps[2:3, :] * former
    gigate[...] = (d_inner * cin[...].astype(F32)).astype(BF16)
    gcin[...] = (d_inner * igate[...].astype(F32)).astype(BF16)
    passed.wait_recv()
    mixed_y.wait_recv()
    gwout[...] = lax.dot_general(grx[...], mixed[...], over_rows, preferred_element_type=F32)
    for n, units in enumerate(leaving):
        await_units(send_sem.at[n], sum(units))
    assert slots_used[0] == recv_sem.shape[0] and len(leaving) <= send_sem.shape[0]


def layer(slices, cap, args):
    rt, rw, resid, og, gate, up, down, ogate, igate, cin, cout, taps, wout = args
    tok, features = resid.shape
    units, channels = gate.shape[1], ogate.shape[1]
    pairs, width = slices // 2, features // 4
    anywhere = pl.BlockSpec(memory_space=pltpu.HBM)
    share = features // slices
    outs = (
        (resid.shape, BF16), (gate.shape, BF16), (down.shape, BF16),
        (ogate.shape, BF16), (ogate.shape, BF16), (ogate.shape, BF16), ((share, channels), F32),
    )
    rows = slices * cap
    sems = 12 * pairs + 2 * slices + 3
    return pl.pallas_call(
        functools.partial(layer_kernel, slices, cap),
        out_shape=tuple(pltpu.VMEM(*out) for out in outs),
        in_specs=[anywhere] * len(args),
        out_specs=[pl.BlockSpec(memory_space=pltpu.VMEM)] * len(outs),
        scratch_shapes=[pltpu.VMEM(arg.shape, arg.dtype) for arg in args]
        + [
            pltpu.VMEM((rows, features), BF16),
            pltpu.VMEM((rows, features), BF16),
            pltpu.VMEM((rows, units), BF16),
            pltpu.VMEM((rows, units), BF16),
            pltpu.VMEM((rows, units), BF16),
            pltpu.VMEM((pairs * cap, tok), BF16),
            pltpu.VMEM((pairs * cap, width), BF16),
            pltpu.VMEM((pairs * cap, width), BF16),
            pltpu.VMEM((rows, features), BF16),
            pltpu.VMEM((2, rows, width), BF16),
            pltpu.VMEM((2, rows, width), BF16),
            pltpu.VMEM((3, pairs * cap, width), BF16),
            pltpu.VMEM((pairs * cap, width), BF16),
            pltpu.VMEM((pairs * cap, width), BF16),
            pltpu.VMEM((tok, features), BF16),
            pltpu.VMEM((2, 8, channels), F32),
            pltpu.VMEM((2, 8, channels), F32),
            pltpu.VMEM((slices * tok, share), BF16),
            pltpu.VMEM((slices * tok, channels), BF16),
            pltpu.SemaphoreType.DMA((5,)),
            pltpu.SemaphoreType.DMA((sems,)),
            pltpu.SemaphoreType.DMA((len(args),)),
        ],
        compiler_params=pltpu.CompilerParams(
            collective_id=0, has_side_effects=True, vmem_limit_bytes=VMEM_LIMIT // 2
        ),
        name="layer",
    )(*(pltpu.with_memory_space_constraint(arg, pltpu.HBM) for arg in args))


def publish_kernel(count, *refs):
    copies = [
        pltpu.make_async_copy(src, dst, refs[-1].at[n])
        for n, (src, dst) in enumerate(zip(refs[:count], refs[count : 2 * count]))
    ]
    for copy in copies:
        copy.start()
    for copy in copies:
        copy.wait()


def publish(arrays):
    return pl.pallas_call(
        functools.partial(publish_kernel, len(arrays)),
        out_shape=tuple(jax.ShapeDtypeStruct(a.shape, a.dtype) for a in arrays),
        in_specs=[pl.BlockSpec(memory_space=pltpu.VMEM)] * len(arrays),
        out_specs=[pl.BlockSpec(memory_space=pl.ANY)] * len(arrays),
        scratch_shapes=[pltpu.SemaphoreType.DMA((len(arrays),))],
        compiler_params=pltpu.CompilerParams(vmem_limit_bytes=VMEM_LIMIT // 4),
        name="publish",
    )(*arrays)


def per_device(
    out_grad, residual, routes, route_weights, w_gate, w_up, w_down,
    out_gate, in_gate, conv_input, conv_out, conv_taps, w_out,
):
    slices = lax.axis_size("sp")
    cap = 5 * out_grad.shape[0] // slices
    results = layer(
        slices, cap,
        (
            routes.T, route_weights.T, residual, out_grad, w_gate[0], w_up[0], w_down[0],
            out_gate, in_gate, conv_input, conv_out, conv_taps, w_out,
        ),
    )
    grad_resid, grad_up, grad_down, *small = publish(results)
    return (grad_resid, grad_up[None], grad_down[None], *small)


def fits_kernels(mesh, tokens):
    slices = mesh.shape["sp"]
    rows = tokens // slices
    powers = slices >= 8 and slices & (slices - 1) == 0
    return mesh.shape["tp"] == 4 and powers and (5 * rows // slices) % 16 == 0


def on_device(mesh, out_grad, *rest):
    tokens = out_grad.shape[0] * mesh.shape["sp"]
    body = per_device if fits_kernels(mesh, tokens) else per_device_general
    return body(out_grad, *rest)


def solution(mesh):
    in_specs = (
        P("sp", None),
        P("sp", None),
        P("sp", None),
        P("sp", None),
        P("sp", None, "tp"),
        P("sp", None, "tp"),
        P("sp", "tp", None),
        P("sp", "tp"),
        P("sp", "tp"),
        P("sp", "tp"),
        P("sp", "tp"),
        P(None, "tp"),
        P("tp", None),
    )
    out_specs = (
        P("sp", None),
        P("sp", None, "tp"),
        P("sp", "tp", None),
        P("sp", "tp"),
        P("sp", "tp"),
        P("sp", "tp"),
        P("sp", "tp"),
    )
    return jax.shard_map(
        functools.partial(on_device, mesh), mesh=mesh, in_specs=in_specs, out_specs=out_specs, check_vma=False
    )
```

```python
import functools
import math

import jax
import jax.numpy as jnp
from jax import lax
from jax.experimental import pallas as pl
from jax.experimental.pallas import tpu as pltpu
from jax.sharding import PartitionSpec as P

epsilon = 1e-06


def with_halo(cells, sides, width):
    for axis, dim in sides:
        count = lax.axis_size(axis)
        ends = count - 1
        head = lax.slice_in_dim(cells, 0, width, axis=dim)
        tail = lax.slice_in_dim(cells, cells.shape[dim] - width, cells.shape[dim], axis=dim)
        cells = jnp.concatenate(
            [
                lax.ppermute(tail, axis, [(i, (i + 1) % count) for i in range(ends)]),
                cells,
                lax.ppermute(head, axis, [((i + 1) % count, i) for i in range(ends)]),
            ],
            axis=dim,
        )
    return cells


def per_device_general(
    out_grad,
    residual,
    routes,
    route_weights,
    w_gate,
    w_up,
    w_down,
    out_gate,
    in_gate,
    conv_input,
    conv_out,
    conv_taps,
    w_out,
):
    tok_rows = out_grad.shape[0]
    features = out_grad.shape[1]
    top_count = routes.shape[1]
    slices = lax.axis_size("sp")
    experts = slices // 2
    capacity = 5 * tok_rows // slices
    n_assign = tok_rows * top_count
    resid_f32 = residual.astype(jnp.float32)
    inv_rms = lax.rsqrt(jnp.mean(resid_f32 * resid_f32, axis=-1, keepdims=True) + epsilon)
    unit_rows = resid_f32 * inv_rms
    normed = unit_rows.astype(jnp.bfloat16)
    weighted = (
        (route_weights[:, :, None] * out_grad.astype(jnp.float32)[:, None, :])
        .astype(jnp.bfloat16)
        .reshape(n_assign, features)
    )
    flat_routes = routes.reshape(-1)
    onehot = (flat_routes[:, None] == jnp.arange(experts, dtype=jnp.int32)[None, :]).astype(
        jnp.int32
    )
    slot_rank = jnp.sum((jnp.cumsum(onehot, axis=0) - onehot) * onehot, axis=1)
    slot_index = flat_routes * capacity + slot_rank
    slot_table = (
        jnp.full((experts * capacity,), n_assign, jnp.int32)
        .at[slot_index]
        .set(jnp.arange(n_assign, dtype=jnp.int32))
    )
    filled = slot_table < n_assign
    safe_index = jnp.where(filled, slot_table, 0)
    send_rows = jnp.where(
        filled[:, None], normed[safe_index // top_count], jnp.zeros((), jnp.bfloat16)
    )
    send_grads = jnp.where(filled[:, None], weighted[safe_index], jnp.zeros((), jnp.bfloat16))
    outgoing = jnp.stack([send_rows, send_grads])
    doubled = jnp.repeat(outgoing.reshape(2, experts, capacity, features), 2, axis=1)
    arrived = lax.all_to_all(doubled, "sp", split_axis=1, concat_axis=1, tiled=True)
    expert_rows = arrived[0].reshape(slices * capacity, features)
    expert_grads = arrived[1].reshape(slices * capacity, features)
    gate_local = w_gate[0]
    up_local = w_up[0]
    down_local = w_down[0]
    pre_gate = jnp.dot(expert_rows, gate_local, preferred_element_type=jnp.float32)
    pre_up = jnp.dot(expert_rows, up_local, preferred_element_type=jnp.float32)
    sigmoid_gate = jax.nn.sigmoid(pre_gate)
    activated = pre_gate * sigmoid_gate
    hidden = (activated * pre_up).astype(jnp.bfloat16)
    d_hidden = lax.dot_general(
        expert_grads, down_local, (((1,), (1,)), ((), ())), preferred_element_type=jnp.float32
    )
    grad_down = lax.dot_general(
        hidden, expert_grads, (((0,), (0,)), ((), ())), preferred_element_type=jnp.float32
    ).astype(jnp.bfloat16)
    d_gate = (d_hidden * pre_up * sigmoid_gate * (1.0 + pre_gate * (1.0 - sigmoid_gate))).astype(
        jnp.bfloat16
    )
    d_up = (d_hidden * activated).astype(jnp.bfloat16)
    grad_up = lax.dot_general(
        expert_rows, d_up, (((0,), (0,)), ((), ())), preferred_element_type=jnp.float32
    ).astype(jnp.bfloat16)
    partial_value = lax.dot_general(
        d_gate, gate_local, (((1,), (1,)), ((), ())), preferred_element_type=jnp.float32
    )
    partial_value = partial_value + lax.dot_general(
        d_up, up_local, (((1,), (1,)), ((), ())), preferred_element_type=jnp.float32
    )
    partial_value = partial_value.astype(jnp.bfloat16).reshape(slices, capacity, features)
    summed = lax.psum_scatter(partial_value, "tp", scatter_dimension=2, tiled=True).astype(
        jnp.float32
    )
    returned = lax.all_to_all(
        summed.astype(jnp.bfloat16), "sp", split_axis=0, concat_axis=0, tiled=True
    )
    columns = returned.shape[2]
    flat_back = returned.reshape(slices * capacity, columns)
    first_index = 2 * flat_routes * capacity + slot_rank
    contrib = flat_back[first_index].astype(jnp.float32) + flat_back[first_index + capacity].astype(
        jnp.float32
    )
    d_normed = jnp.sum(contrib.reshape(tok_rows, top_count, columns), axis=1)
    col_start = lax.axis_index("tp") * columns
    unit_part = lax.dynamic_slice_in_dim(unit_rows, col_start, columns, 1)
    grad_part = lax.dynamic_slice_in_dim(out_grad, col_start, columns, 1).astype(jnp.float32)
    row_dots = lax.psum(jnp.sum(unit_part * d_normed, axis=-1), "tp")
    row_mean = row_dots[:, None] / features
    resid_part = (grad_part + inv_rms * (d_normed - unit_part * row_mean)).astype(jnp.bfloat16)
    grad_resid = lax.all_gather(resid_part, "tp", axis=1, tiled=True)
    d_mix = lax.dot_general(
        grad_resid, w_out, (((1,), (1,)), ((), ())), preferred_element_type=jnp.float32
    )
    conv_f32 = conv_out.astype(jnp.float32)
    gate_f32 = out_gate.astype(jnp.float32)
    grad_out_gate = (d_mix * conv_f32).astype(jnp.bfloat16)
    d_conv = d_mix * gate_f32
    padded = with_halo(d_conv.astype(jnp.bfloat16), (("sp", 0),), 1).astype(d_conv.dtype)
    d_inner = conv_taps[0] * padded[2:] + conv_taps[1] * padded[1:-1] + conv_taps[2] * padded[:-2]
    grad_in_gate = (d_inner * conv_input.astype(jnp.float32)).astype(jnp.bfloat16)
    grad_conv_input = (d_inner * in_gate.astype(jnp.float32)).astype(jnp.bfloat16)
    mixed = (gate_f32 * conv_f32).astype(jnp.bfloat16)
    grad_w_out = lax.psum_scatter(
        lax.dot_general(
            grad_resid, mixed, (((0,), (0,)), ((), ())), preferred_element_type=jnp.float32
        ),
        "sp",
        scatter_dimension=0,
        tiled=True,
    )
    return (
        grad_resid,
        grad_up[None],
        grad_down[None],
        grad_out_gate,
        grad_in_gate,
        grad_conv_input,
        grad_w_out,
    )


MESH = pl.DeviceIdType.MESH
BF16 = jnp.bfloat16
F32 = jnp.float32
VMEM_LIMIT = 60 * 1024 * 1024


def place():
    sp, tp = lax.axis_index("sp"), lax.axis_index("tp")
    return sp, tp, lax.div(sp, 2), lax.rem(sp, 2), lax.div(tp, 2), lax.rem(tp, 2)


def greet(peers):
    barrier = pltpu.get_barrier_semaphore()
    for peer in peers:
        pl.semaphore_signal(barrier, inc=1, device_id=peer, device_id_type=MESH)
    return lambda: pl.semaphore_wait(barrier, len(peers))


def columns_of(index, width):
    return pl.ds(pl.multiple_of(index * width, width), width)


def rows_of(index, height):
    return pl.ds(pl.multiple_of(index * height, height), height)


def layer_kernel(
    slices, cap,
    rt_hbm, rw_hbm, resid_hbm, og_hbm, gate_hbm, up_hbm, down_hbm,
    ogate_hbm, igate_hbm, cin_hbm, cout_hbm, taps_hbm, wout_hbm,
    gresid, gup, gdown, gogate, gigate, gcin, gwout,
    rt, rw, resid, og, gate, up, down, ogate, igate, cin, cout, taps, wout,
    rows, grads, hidden, d_gate, d_up, sel, send_rows, send_grads,
    gate_t, up_t, down_t, part, sib, pairsum, plane, zsend, ret, dn, edge_out, edge_in, grx, mixed,
    send_sem, recv_sem, in_sem,
):
    sp, tp, z, y, x, c = place()
    pairs = slices // 2
    tok, features = resid.shape
    units = gate.shape[1]
    width = features // 4
    sibling = (sp, 2 * x + 1 - c)
    x_peer = (sp, 2 * (1 - x) + c)
    y_peer = (2 * z + 1 - y, tp)
    x_other = (sp, 2 * (1 - x) + 1 - c)
    diagonal = (2 * z + 1 - y, 2 * (1 - x) + c)
    sp_peers = [(lax.rem(sp + k, slices), tp) for k in range(1, slices)]
    ready = greet(sp_peers + [sibling, x_peer, x_other, diagonal])

    def pair_of(k):
        code, pair, bit = k ^ (k >> 1), 0, 1
        while bit < pairs:
            pair = pair + bit * lax.rem(lax.rem(lax.div(z, bit), 2) + (code // bit) % 2, 2)
            bit *= 2
        return pair

    def fetch(n, src, dst):
        copy = pltpu.make_async_copy(src, dst, in_sem.at[n])
        copy.start()
        return copy

    first = [
        fetch(n, src, dst)
        for n, (src, dst) in enumerate(
            ((resid_hbm, resid), (rt_hbm, rt), (rw_hbm, rw), (og_hbm, og))
        )
    ]
    weights = [
        fetch(4 + n, src, dst)
        for n, (src, dst) in enumerate(((down_hbm, down), (gate_hbm, gate), (up_hbm, up)))
    ]
    gates = [
        fetch(7 + n, src, dst)
        for n, (src, dst) in enumerate(
            (
                (ogate_hbm, ogate), (cout_hbm, cout), (wout_hbm, wout),
                (igate_hbm, igate), (cin_hbm, cin), (taps_hbm, taps),
            )
        )
    ]
    unit_cols = gate.shape[1]
    slots_used, leaving = [0], [[]]

    def units_of(ref):
        return math.prod(ref.shape) * jnp.dtype(ref.dtype).itemsize // (2 * unit_cols)

    def await_units(sem, units):
        assert units <= gate.shape[0]
        like = gate.at[pl.ds(0, units), :]
        pltpu.make_async_copy(like, like, sem).wait()

    class Batch:
        def __init__(self):
            self.slot, self.units = slots_used[0], 0
            slots_used[0] += 1

        def wait_recv(self):
            await_units(recv_sem.at[self.slot], self.units)

    def send(src, dst, peer, batch=None):
        batch = batch or Batch()
        units = units_of(src)
        batch.units += units
        if sum(leaving[-1]) + units > gate.shape[0]:
            leaving.append([])
        leaving[-1].append(units)
        pltpu.make_async_remote_copy(
            src_ref=src, dst_ref=dst, send_sem=send_sem.at[len(leaving) - 1],
            recv_sem=recv_sem.at[batch.slot], device_id=peer, device_id_type=MESH,
        ).start()
        return batch

    def block(pair, yy, xx, cc):
        return (rows_of(2 * pair + yy, cap), columns_of(2 * xx + cc, width))

    for copy in first:
        copy.wait()
    grid_r = lax.broadcasted_iota(jnp.int32, (tok, tok), 0)
    grid_c = lax.broadcasted_iota(jnp.int32, (tok, tok), 1)
    earlier = (grid_r < grid_c).astype(F32).astype(BF16)
    slot = lax.broadcasted_iota(jnp.int32, (cap, tok), 0).astype(F32)
    r32 = resid[...].astype(F32)
    inv_rms = lax.rsqrt(jnp.mean(r32 * r32, axis=-1, keepdims=True) + epsilon)
    mine = columns_of(tp, width)
    normed = (resid[:, mine].astype(F32) * inv_rms).astype(BF16)
    cot = og[:, mine]

    def choose(e):
        named = (rt[...] == e).astype(F32)
        mask = jnp.sum(named, axis=0, keepdims=True)
        weight = jnp.sum(named * rw[...], axis=0, keepdims=True)
        rank = jnp.dot(
            jnp.broadcast_to(mask, (8, tok)).astype(BF16), earlier, preferred_element_type=F32
        )[0:1]
        pick = jnp.where((rank == slot) & (mask > 0.5), 1.0, 0.0)
        slot_weight = jnp.sum(pick * weight, axis=1, keepdims=True)
        pick = pick.astype(BF16)
        sel[rows_of(e, cap), :] = pick
        return pick, slot_weight

    both, arriving = (rows, grads), {}
    outs = [{} for _ in range(pairs)]
    near_rows = [Batch() for _ in range(pairs)]

    def spread(k, a):
        out, ref, at = outs[k], both[a], block(pair_of(k), y, x, c)
        if k:
            arriving[k, a].wait_recv()
            out["x", a] = send(ref.at[at], ref.at[at], x_peer)
        out["y", a] = send(ref.at[at], ref.at[at], y_peer)
        if k:
            send(ref.at[at], ref.at[at], sibling, near_rows[k])
        elif a == 0:
            at = block(z, y, 1 - x, c)
            out["d", a] = send(ref.at[at], ref.at[at], y_peer)

    def dispatch(k):
        e = pair_of(k)
        pick, slot_weight = choose(e)
        here, home = rows_of(e, cap), block(z, y, x, c)
        send_rows[here, :] = jnp.dot(pick, normed, preferred_element_type=F32).astype(BF16)
        arriving[k, 0] = send(send_rows.at[here, :], rows.at[home], (2 * e + y, tp))
        send_grads[here, :] = (
            slot_weight * jnp.dot(pick, cot, preferred_element_type=F32)
        ).astype(BF16)
        arriving[k, 1] = send(send_grads.at[here, :], grads.at[home], (2 * e + y, tp))

    pick, slot_weight = choose(z)
    own_rows = rows_of(sp, cap)
    grads[own_rows, :] = (
        slot_weight * jnp.dot(pick, og[...], preferred_element_type=F32)
    ).astype(BF16)
    ready()
    spread(0, 1)
    dispatch(1)
    rows[own_rows, :] = jnp.dot(
        pick, (r32 * inv_rms).astype(BF16), preferred_element_type=F32
    ).astype(BF16)
    spread(0, 0)
    for k in range(2, pairs):
        dispatch(k)

    def got_x(k, a):
        out, ref, at = outs[k], both[a], block(pair_of(k), y, 1 - x, c)
        out["x", a].wait_recv()
        if a == 0:
            out["d", a] = send(ref.at[at], ref.at[at], y_peer)
        send(ref.at[at], ref.at[at], sibling, near_rows[k])

    def got_y(k, a):
        out, ref, at = outs[k], both[a], block(pair_of(k), 1 - y, x, c)
        out["y", a].wait_recv()
        if a == 1:
            out["d", a] = send(ref.at[at], ref.at[at], x_peer)
        send(ref.at[at], ref.at[at], sibling, near_rows[k])

    def got_d(k, a):
        out, ref, at = outs[k], both[a], block(pair_of(k), 1 - y, 1 - x, c)
        out["d", a].wait_recv()
        send(ref.at[at], ref.at[at], sibling, near_rows[k])

    held, halves, moved, back = {}, {}, {}, Batch()

    def experts(k, step):
        at = rows_of(pair_of(k), 2 * cap)
        if step == 0:
            near_rows[k].wait_recv()
            held["gate"] = jnp.dot(rows[at, :], gate[...], preferred_element_type=F32)
        elif step == 1:
            held["up"] = jnp.dot(rows[at, :], up[...], preferred_element_type=F32)
        else:
            pre_gate, pre_up = held["gate"], held["up"]
            d_hidden = jnp.dot(grads[at, :], down_t[...], preferred_element_type=F32)
            sigmoid_gate = jax.nn.sigmoid(pre_gate)
            activated = pre_gate * sigmoid_gate
            hidden[at, :] = (activated * pre_up).astype(BF16)
            d_gate[at, :] = (
                d_hidden * pre_up * sigmoid_gate * (1.0 + pre_gate * (1.0 - sigmoid_gate))
            ).astype(BF16)
            d_up[at, :] = (d_hidden * activated).astype(BF16)

    def partials(k, step):
        at, h = rows_of(pair_of(k), 2 * cap), x if step else 1 - x
        cols = columns_of(h, 2 * width)
        part[at, cols] = (
            jnp.dot(d_gate[at, :], gate_t[:, cols], preferred_element_type=F32)
            + jnp.dot(d_up[at, :], up_t[:, cols], preferred_element_type=F32)
        ).astype(BF16)
        halves[k, step] = send(
            part.at[at, columns_of(2 * h + 1 - c, width)], sib.at[h, at, :], sibling
        )

    def reduce_cores(k, step):
        pair, h = pair_of(k), x if step else 1 - x
        at = rows_of(pair, 2 * cap)
        halves[k, step].wait_recv()
        pairsum[h, at, :] = (
            part[at, columns_of(2 * h + c, width)].astype(F32) + sib[h, at, :].astype(F32)
        ).astype(BF16)
        same, other = rows_of(2 * pair + y, cap), rows_of(2 * pair + 1 - y, cap)
        slots = rows_of(pair, cap)
        if step:
            send(pairsum.at[h, other, :], plane.at[1, slots, :], y_peer, moved[k])
        else:
            moved[k] = Batch()
            send(pairsum.at[h, other, :], plane.at[2, slots, :], diagonal, moved[k])
            send(pairsum.at[h, same, :], plane.at[0, slots, :], x_peer, moved[k])

    def reduce_plane(k):
        pair = pair_of(k)
        slots = rows_of(pair, cap)
        moved[k].wait_recv()
        total = (
            pairsum[x, rows_of(2 * pair + y, cap), :].astype(F32)
            + plane[0, slots, :].astype(F32)
            + plane[1, slots, :].astype(F32)
            + plane[2, slots, :].astype(F32)
        ).astype(BF16)
        if k:
            zsend[slots, :] = total
            send(zsend.at[slots, :], ret.at[rows_of(z, cap), :], (2 * pair + y, tp), back)
        else:
            ret[slots, :] = total

    over_rows = (((0,), (0,)), ((), ()))

    def down_chunk(n):
        at = slice(n * units // 2, (n + 1) * units // 2)
        gdown[at, :] = lax.dot_general(
            hidden[:, at], grads[...], over_rows, preferred_element_type=F32
        ).astype(BF16)

    def up_chunk(n):
        at = slice(n * features // 4, (n + 1) * features // 4)
        gup[at, :] = lax.dot_general(
            rows[:, at], d_up[...], over_rows, preferred_element_type=F32
        ).astype(BF16)

    own = rows_of(sp, tok)

    mixed_z, mixed_y = Batch(), Batch()

    def share_mixed():
        for copy in gates:
            copy.wait()
        mixed[own, :] = (ogate[...].astype(F32) * cout[...].astype(F32)).astype(BF16)
        for k in range(1, pairs):
            peer = (2 * pair_of(k) + y, tp)
            send(mixed.at[own, :], mixed.at[own, :], peer, mixed_z)

    def relay_mixed():
        mixed_z.wait_recv()
        for k in range(pairs):
            at = rows_of(2 * pair_of(k) + y, tok)
            send(mixed.at[at, :], mixed.at[at, :], y_peer, mixed_y)

    def turn(n):
        weights[n].wait()
        src, dst = ((down, down_t), (gate, gate_t), (up, up_t))[n]
        dst[...] = src[...].T

    turn(0)
    got_y(0, 1)
    spread(1, 0)
    spread(1, 1)
    got_y(0, 0)
    turn(1)
    last = pairs - 1
    for k in range(1, pairs):
        if k == 1:
            got_d(0, 0)
            got_y(k, 0)
            got_x(k, 0)
            got_y(k, 1)
            got_d(0, 1)
            turn(2)
            spread(2, 0)
            spread(2, 1)
            got_x(k, 1)
            experts(k - 1, 0)
            experts(k - 1, 1)
        elif k == 2:
            got_y(k, 0)
            experts(k - 1, 0)
            got_x(k, 0)
            got_y(k, 1)
            experts(k - 1, 1)
            got_x(k, 1)
        else:
            got_y(k, 0)
            got_x(k, 0)
            got_y(k, 1)
            got_x(k, 1)
            got_d(k - 1, 0)
            got_d(k - 1, 1)
            reduce_cores(k - 2, 0)
            reduce_cores(k - 2, 1)
            experts(k - 1, 0)
            experts(k - 1, 1)
        if k == last:
            got_d(k, 0)
            got_d(k, 1)
        if k + 2 < pairs:
            spread(k + 2, 0)
        if k + 2 == pairs:
            share_mixed()
        experts(k - 1, 2)
        partials(k - 1, 0)
        if k + 2 < pairs:
            spread(k + 2, 1)
        if k == 1:
            got_d(k, 0)
            got_d(k, 1)
        partials(k - 1, 1)
    experts(last, 0)
    experts(last, 1)
    reduce_cores(last - 1, 0)
    reduce_cores(last - 1, 1)
    experts(last, 2)
    partials(last, 0)
    partials(last, 1)
    for k in range(1, last - 1):
        reduce_plane(k)
    up_chunk(0)
    reduce_cores(last, 0)
    reduce_cores(last, 1)
    reduce_cores(0, 0)
    reduce_cores(0, 1)
    up_chunk(1)
    down_chunk(0)
    reduce_plane(last - 1)
    down_chunk(1)
    reduce_plane(last)
    up_chunk(2)
    up_chunk(3)
    reduce_plane(0)
    relay_mixed()

    back.wait_recv()
    dn[:, mine] = lax.dot_general(
        sel[...], ret[...], over_rows, preferred_element_type=F32
    ).astype(BF16)
    half, quarter = tok // 2, tok // 4
    far, beyond = columns_of(2 * (1 - x) + c, width), columns_of(1 - x, 2 * width)
    share = features // slices
    leading, trailing = Batch(), Batch()
    here, there = rows_of(2 * x + c, quarter), rows_of(2 * x + 1 - c, quarter)
    away = rows_of(1 - x, half)

    def share_rows(at, cols, peer, batch=None):
        return send(dn.at[at, cols], dn.at[at, cols], peer, batch)

    def resid_rows(at):
        r_part = resid[at, :].astype(F32)
        inv_part = lax.rsqrt(jnp.mean(r_part * r_part, axis=-1, keepdims=True) + epsilon)
        unit = r_part * inv_part
        d_normed = dn[at, :].astype(F32)
        row_mean = jnp.mean(unit * d_normed, axis=-1, keepdims=True)
        gresid[at, :] = (
            og[at, :].astype(F32) + inv_part * (d_normed - unit * row_mean)
        ).astype(BF16)

    share_rows(rows_of(2 * (1 - x) + 1 - c, quarter), mine, x_other, leading)
    share_rows(rows_of(2 * (1 - x) + c, quarter), mine, x_peer, leading)
    share_rows(there, mine, sibling, leading)
    rest = share_rows(rows_of(x, half), mine, x_peer)
    share_rows(here, mine, sibling, trailing)
    share_rows(away, mine, sibling, trailing)

    def piece(origin, xx):
        return grx.at[rows_of(4 * origin + 2 * xx + c, quarter), :]

    def peer_of(j, flip):
        return 2 * pair_of(j) + (1 - y if flip else y)

    leading.wait_recv()
    resid_rows(here)
    across, crossed, passed = {}, {}, Batch()
    for j, flip in [(j, f) for j in range(pairs - 1, 0, -1) for f in range(2)] + [(0, 1)]:
        peer = peer_of(j, flip)
        src = gresid.at[here, columns_of(peer, share)]
        across[j, flip] = send(src, piece(sp, x), (peer, tp))
    share_rows(here, beyond, sibling, trailing)
    rest.wait_recv()
    share_rows(away, far, sibling, trailing)
    trailing.wait_recv()
    resid_rows(there)
    resid_rows(away)
    d_mix = lax.dot_general(
        gresid[...], wout[...], (((1,), (1,)), ((), ())), preferred_element_type=F32
    )
    d_conv = d_mix * ogate[...].astype(F32)
    edge_out[0] = d_conv[tok - 8 :]
    edge_out[1] = d_conv[:8]
    edges = Batch()
    send(edge_out.at[0], edge_in.at[0], sp_peers[0], edges)
    send(edge_out.at[1], edge_in.at[1], sp_peers[-1], edges)
    gogate[...] = (d_mix * cout[...].astype(F32)).astype(BF16)
    grx[own, :] = gresid[:, columns_of(sp, share)]
    arrivals = [(0, 1), (1, 0), (1, 1)]
    arrivals += [(j, f) for j in range(pairs - 1, 1, -1) for f in range(2)]
    for j, flip in arrivals:
        across[j, flip].wait_recv()
        got = piece(peer_of(j, flip), x)
        crossed[j, flip] = send(got, got, x_peer)
        send(got, got, sibling, passed)
    for j, flip in arrivals:
        crossed[j, flip].wait_recv()
        got = piece(peer_of(j, flip), 1 - x)
        send(got, got, sibling, passed)
    edges.wait_recv()
    before = jnp.where(sp > 0, edge_in[0, 7:8, :], 0.0)
    after = jnp.where(sp < slices - 1, edge_in[1, 0:1, :], 0.0)
    at = lax.broadcasted_iota(jnp.int32, d_conv.shape, 0)
    later = jnp.where(at == tok - 1, after, pltpu.roll(d_conv, tok - 1, 0))
    former = jnp.where(at == 0, before, pltpu.roll(d_conv, 1, 0))
    d_inner = taps[0:1, :] * later + taps[1:2, :] * d_conv + taps[2:3, :] * former
    gigate[...] = (d_inner * cin[...].astype(F32)).astype(BF16)
    gcin[...] = (d_inner * igate[...].astype(F32)).astype(BF16)
    passed.wait_recv()
    mixed_y.wait_recv()
    gwout[...] = lax.dot_general(grx[...], mixed[...], over_rows, preferred_element_type=F32)
    for n, units in enumerate(leaving):
        await_units(send_sem.at[n], sum(units))
    assert slots_used[0] == recv_sem.shape[0] and len(leaving) <= send_sem.shape[0]


def layer(slices, cap, args):
    rt, rw, resid, og, gate, up, down, ogate, igate, cin, cout, taps, wout = args
    tok, features = resid.shape
    units, channels = gate.shape[1], ogate.shape[1]
    pairs, width = slices // 2, features // 4
    anywhere = pl.BlockSpec(memory_space=pltpu.HBM)
    share = features // slices
    outs = (
        (resid.shape, BF16), (gate.shape, BF16), (down.shape, BF16),
        (ogate.shape, BF16), (ogate.shape, BF16), (ogate.shape, BF16), ((share, channels), F32),
    )
    rows = slices * cap
    sems = 12 * pairs + 2 * slices + 2
    return pl.pallas_call(
        functools.partial(layer_kernel, slices, cap),
        out_shape=tuple(pltpu.VMEM(*out) for out in outs),
        in_specs=[anywhere] * len(args),
        out_specs=[pl.BlockSpec(memory_space=pltpu.VMEM)] * len(outs),
        scratch_shapes=[pltpu.VMEM(arg.shape, arg.dtype) for arg in args]
        + [
            pltpu.VMEM((rows, features), BF16),
            pltpu.VMEM((rows, features), BF16),
            pltpu.VMEM((rows, units), BF16),
            pltpu.VMEM((rows, units), BF16),
            pltpu.VMEM((rows, units), BF16),
            pltpu.VMEM((pairs * cap, tok), BF16),
            pltpu.VMEM((pairs * cap, width), BF16),
            pltpu.VMEM((pairs * cap, width), BF16),
            pltpu.VMEM((units, features), BF16),
            pltpu.VMEM((units, features), BF16),
            pltpu.VMEM((features, units), BF16),
            pltpu.VMEM((rows, features), BF16),
            pltpu.VMEM((2, rows, width), BF16),
            pltpu.VMEM((2, rows, width), BF16),
            pltpu.VMEM((3, pairs * cap, width), BF16),
            pltpu.VMEM((pairs * cap, width), BF16),
            pltpu.VMEM((pairs * cap, width), BF16),
            pltpu.VMEM((tok, features), BF16),
            pltpu.VMEM((2, 8, channels), F32),
            pltpu.VMEM((2, 8, channels), F32),
            pltpu.VMEM((slices * tok, share), BF16),
            pltpu.VMEM((slices * tok, channels), BF16),
            pltpu.SemaphoreType.DMA((5,)),
            pltpu.SemaphoreType.DMA((sems,)),
            pltpu.SemaphoreType.DMA((len(args),)),
        ],
        compiler_params=pltpu.CompilerParams(
            collective_id=0, has_side_effects=True, vmem_limit_bytes=2 * VMEM_LIMIT // 3
        ),
        name="layer",
    )(*(pltpu.with_memory_space_constraint(arg, pltpu.HBM) for arg in args))


def publish_kernel(count, *refs):
    copies = [
        pltpu.make_async_copy(src, dst, refs[-1].at[n])
        for n, (src, dst) in enumerate(zip(refs[:count], refs[count : 2 * count]))
    ]
    for copy in copies:
        copy.start()
    for copy in copies:
        copy.wait()


def publish(arrays):
    return pl.pallas_call(
        functools.partial(publish_kernel, len(arrays)),
        out_shape=tuple(jax.ShapeDtypeStruct(a.shape, a.dtype) for a in arrays),
        in_specs=[pl.BlockSpec(memory_space=pltpu.VMEM)] * len(arrays),
        out_specs=[pl.BlockSpec(memory_space=pl.ANY)] * len(arrays),
        scratch_shapes=[pltpu.SemaphoreType.DMA((len(arrays),))],
        compiler_params=pltpu.CompilerParams(vmem_limit_bytes=VMEM_LIMIT // 4),
        name="publish",
    )(*arrays)


def per_device(
    out_grad, residual, routes, route_weights, w_gate, w_up, w_down,
    out_gate, in_gate, conv_input, conv_out, conv_taps, w_out,
):
    slices = lax.axis_size("sp")
    cap = 5 * out_grad.shape[0] // slices
    results = layer(
        slices, cap,
        (
            routes.T, route_weights.T, residual, out_grad, w_gate[0], w_up[0], w_down[0],
            out_gate, in_gate, conv_input, conv_out, conv_taps, w_out,
        ),
    )
    grad_resid, grad_up, grad_down, *small = publish(results)
    return (grad_resid, grad_up[None], grad_down[None], *small)


def fits_kernels(mesh, tokens):
    slices = mesh.shape["sp"]
    rows = tokens // slices
    powers = slices >= 8 and slices & (slices - 1) == 0
    return mesh.shape["tp"] == 4 and powers and (5 * rows // slices) % 16 == 0


def on_device(mesh, out_grad, *rest):
    tokens = out_grad.shape[0] * mesh.shape["sp"]
    body = per_device if fits_kernels(mesh, tokens) else per_device_general
    return body(out_grad, *rest)


def solution(mesh):
    in_specs = (
        P("sp", None),
        P("sp", None),
        P("sp", None),
        P("sp", None),
        P("sp", None, "tp"),
        P("sp", None, "tp"),
        P("sp", "tp", None),
        P("sp", "tp"),
        P("sp", "tp"),
        P("sp", "tp"),
        P("sp", "tp"),
        P(None, "tp"),
        P("tp", None),
    )
    out_specs = (
        P("sp", None),
        P("sp", None, "tp"),
        P("sp", "tp", None),
        P("sp", "tp"),
        P("sp", "tp"),
        P("sp", "tp"),
        P("sp", "tp"),
    )
    return jax.shard_map(
        functools.partial(on_device, mesh), mesh=mesh, in_specs=in_specs, out_specs=out_specs, check_vma=False
    )
```
